256 devices in a mesh: sp: 64 (over z, y, core), tp: 4 (over x).
Axes of the slice: x: 4, y: 4, z: 8, core: 2. Of those that a mesh axis runs over, the one named last changes fastest.
Arguments:
- moe_input: bfloat16 [8192, 2048], P('sp', 'tp'), may hold values from -6 to 6
- cotangent: bfloat16 [8192, 2048], P('sp', 'tp'), may hold values from -16 to 16
- expert_ids: int32 [8192, 2], P('sp'), may hold values from 0 to 63, as said below
- routing_weights: float32 [8192, 2], P('sp'), may hold values from 0.1 to 0.6
- gate_weight: bfloat16 [64, 2048, 1024], P('sp', None, 'tp'), may hold values from -0.125 to 0.125
- up_weight: bfloat16 [64, 2048, 1024], P('sp', None, 'tp'), may hold values from -0.125 to 0.125
- down_weight: bfloat16 [64, 1024, 2048], P('sp', 'tp'), may hold values from -0.1875 to 0.1875
- inner_x: bfloat16 [8192, 4096], P('sp', 'tp'), may hold values from -6 to 6
- inner_b: bfloat16 [8192, 256], P('sp', 'tp'), may hold values from -6 to 6
- inner_c: bfloat16 [8192, 256], P('sp', 'tp'), may hold values from -6 to 6
- gate_z: bfloat16 [8192, 4096], P('sp', 'tp'), may hold values from -6 to 6
- step_raw: float32 [8192, 64], P('sp', 'tp'), may hold values from -30 to 2
- decay_rate: float32 [64], P('tp'), may hold values from 1 to 16
- skip_weight: float32 [64], P('tp'), may hold values from 0.1 to 1.9
- norm_gain: float32 [4096], P('tp'), may hold values from 0.1 to 1.9
- w_out: bfloat16 [2048, 4096], P(None, 'tp'), may hold values from -0.09375 to 0.09375
Outputs:
- gate_weight_gradient: bfloat16 [64, 2048, 1024], P('sp', None, 'tp')
- up_weight_gradient: bfloat16 [64, 2048, 1024], P('sp', None, 'tp')
- down_weight_gradient: bfloat16 [64, 1024, 2048], P('sp', 'tp')
- grad_out: float32 [2048, 4096], P('sp', 'tp')
- grad_inner_x: bfloat16 [8192, 4096], P('sp', 'tp')
- grad_inner_b: float32 [8192, 256], P('sp', 'tp')
- grad_inner_c: float32 [8192, 256], P('sp', 'tp')
- grad_gate_z: bfloat16 [8192, 4096], P('sp', 'tp')
- grad_step_raw: float32 [8192, 64], P('sp', 'tp')
The draws below stay inside these ranges and needn't reach their ends.
Inputs may be any that keep to these rules, and one draw needn't show every extreme that they name: `expert_ids`: the two entries of a row differ and lie in the same group of 16 consecutive experts. In each aligned block of 128 rows no expert is named more than 8 times; one group of experts, the same for all blocks, takes exactly half of every block's rows, and each of its experts is named exactly 8 times in every block.
All inputs are finite; a program needn't handle non-finite values.
Results may differ from the reference program's by a relative error of at most 0.015.
Values may be sent and summed in bfloat16 or wider, within the bound.
A program may use at most 128 MiB of HBM per device.

```python
import math
from functools import partial
import jax
import jax.numpy as jnp
from jax import lax

D = 2048
HEADS = 64
HEAD_DIM = 64
GROUPS = 4
STATE = 64
SPAN = 128
FF = 1024
MOE_GROUPS = 4
TOP = 2
EXP_DEV = 1
TOKENS_PER_SHARD = 128
TOKENS = 8192
INNER = 4096
EXPERTS = 64
N_SP = 64
N_TP = 4


def head_laws(key):
    keys = jax.random.split(jax.random.fold_in(key, 101), 4)
    share = 0.5
    quick_head = jax.random.uniform(keys[0], (HEADS,), jnp.float32) < share
    decays = jnp.exp(jax.random.uniform(keys[1], (HEADS,), jnp.float32, 0.0, math.log(16.0)))
    quick = jnp.exp(jax.random.uniform(keys[2], (HEADS,), jnp.float32, math.log(1.0 / 120.0), math.log(1.0 / 40.0)))
    lasting = jnp.exp(jax.random.uniform(keys[3], (HEADS,), jnp.float32, math.log(0.1 / TOKENS), math.log(0.8 / TOKENS)))
    target = jnp.where(quick_head, quick, lasting)
    return (decays, target / decays)


def draw_decay_rate(key, part):
    return head_laws(key)[0]


def draw_step_raw(key, part):
    base_step = head_laws(key)[1]
    offsets = jnp.log(jnp.expm1(base_step))
    keys = jax.random.split(jax.random.fold_in(key, 202), 2)
    blocks = TOKENS // SPAN
    noise = jax.random.truncated_normal(keys[0], -2.5, 2.5, (TOKENS, HEADS), jnp.float32) * 0.7
    level = jax.random.uniform(keys[1], (blocks, 1, 1), jnp.float32, -0.7, 0.7)
    field = noise.reshape(blocks, SPAN, HEADS) + level
    return field.reshape(TOKENS, HEADS) + offsets[None, :]


def draw_expert_ids(key, part):
    expert_list = EXP_DEV * N_SP
    per_group = expert_list // MOE_GROUPS
    blocks = N_SP
    keys = jax.random.split(jax.random.fold_in(key, 303), 5)

    def shuffled(key_one):
        return jax.random.permutation(key_one, TOKENS_PER_SHARD)

    def mixed_table(key_one):
        return jax.random.permutation(key_one, per_group)
    full_group = jax.random.randint(keys[0], (), 0, MOE_GROUPS)
    order = jax.vmap(shuffled)(jax.random.split(keys[1], blocks))
    position = jnp.arange(TOKENS_PER_SHARD, dtype=jnp.int32)
    others = (full_group + 1 + jax.random.randint(keys[2], (blocks, TOKENS_PER_SHARD), 0, MOE_GROUPS - 1)) % MOE_GROUPS
    group_at = jnp.where(position[None, :] < TOKENS_PER_SHARD // 2, full_group, others).astype(jnp.int32)
    onehot = (group_at[:, :, None] == jnp.arange(MOE_GROUPS, dtype=jnp.int32)[None, None, :]).astype(jnp.int32)
    ranks = jnp.sum((jnp.cumsum(onehot, axis=1) - onehot) * onehot, axis=2)
    routing_tables = jax.vmap(mixed_table)(jax.random.split(keys[3], blocks * MOE_GROUPS)).reshape(blocks, MOE_GROUPS, per_group)
    offsets = jax.random.randint(keys[4], (blocks, MOE_GROUPS), 1, per_group)
    table_at = jnp.take_along_axis(routing_tables, jnp.broadcast_to(group_at[:, :, None], (blocks, TOKENS_PER_SHARD, per_group)), axis=1)
    shift_at = jnp.take_along_axis(offsets, group_at, axis=1)
    first = jnp.take_along_axis(table_at, (ranks % per_group)[:, :, None], axis=2)[:, :, 0]
    second = jnp.take_along_axis(table_at, ((ranks + shift_at) % per_group)[:, :, None], axis=2)[:, :, 0]
    chosen = jnp.stack([first, second], axis=2) + group_at[:, :, None] * per_group
    row_index = jnp.arange(blocks, dtype=jnp.int32)[:, None]
    placed = jnp.zeros((blocks, TOKENS_PER_SHARD, TOP), jnp.int32).at[row_index, order].set(chosen)
    return placed.reshape(blocks * TOKENS_PER_SHARD, TOP)


def strengthened(values, key, source, target, shards_of, factor):
    def block_of(dim):
        return (jnp.arange(values.shape[dim]) // (values.shape[dim] // shards_of)).reshape((-1,) + (1,) * (values.ndim - 1 - dim))

    near = jax.random.permutation(key, shards_of)[block_of(target)]
    second = (block_of(target) + shards_of // 2) % shards_of
    return jnp.where((block_of(source) == near) | (block_of(source) == second), factor * values, values)


def steps_of(stream_key, shape, pieces, smallest, top_value):
    gain, own = 1.0, jax.random.fold_in(stream_key, 6)
    for dim, blocks in pieces:
        draws = jnp.exp(jax.random.uniform(jax.random.fold_in(own, dim), (blocks,), jnp.float32, smallest / len(pieces), top_value / len(pieces)))
        gain = gain * jnp.repeat(draws, shape[dim] // blocks).reshape([-1 if axis == dim else 1 for axis in range(len(shape))])
    return gain


def gaussian(stream_key, dims, deviation, reach, cuts=(), held_as=jnp.bfloat16):
    array = deviation * jax.random.normal(stream_key, dims, jnp.float32)
    if cuts:
        array = array * steps_of(stream_key, dims, cuts, -0.22, 0.18)
    return jnp.clip(array, -reach, reach).astype(held_as)


def noise_with(key, dims, spread, reach, cuts, heavy, kind=jnp.bfloat16):
    array = spread * jax.random.normal(key, dims, jnp.float32)
    if cuts:
        array = array * steps_of(key, dims, cuts, -0.22, 0.18)
    return jnp.clip(strengthened(array, jax.random.fold_in(key, 3), *heavy), -reach, reach).astype(kind)


def setup_inputs(seed: int = 0) -> dict:
    streams_of = jax.random.split(jax.random.key(seed), 17)
    moe_input = gaussian(streams_of[0], (TOKENS, D), 1.0, 6.0, ((0, 64), (1, 4)))
    cotangent = noise_with(streams_of[1], (TOKENS, D), 1.0, 16.0, ((0, 64), (1, 4)), (0, 1, 64, 4.0))
    expert_ids = draw_expert_ids(jax.random.fold_in(streams_of[16], 71), 0)
    routing_weights = jnp.clip(0.1 + 0.5 * jax.random.uniform(streams_of[3], (TOKENS, TOP), jnp.float32) ** steps_of(streams_of[3], (TOKENS, TOP), ((0, 64),), -0.2, 0.2), 0.1, 0.6)
    gate_weight = gaussian(streams_of[4], (EXPERTS, D, FF), D ** -0.5, 0.125, ((0, 64), (2, 4)))
    up_weight = gaussian(streams_of[5], (EXPERTS, D, FF), D ** -0.5, 0.125, ((0, 64), (2, 4)))
    down_weight = gaussian(streams_of[6], (EXPERTS, FF, D), FF ** -0.5, 0.1875, ((0, 64), (1, 4)))
    inner_x = gaussian(streams_of[7], (TOKENS, INNER), 1.0, 6.0, ((0, 64), (1, 4)))
    inner_b = gaussian(streams_of[8], (TOKENS, GROUPS * STATE), 1.0, 6.0, ((0, 64), (1, 4)))
    inner_c = gaussian(streams_of[9], (TOKENS, GROUPS * STATE), 1.0, 6.0, ((0, 64), (1, 4)))
    gate_z = gaussian(streams_of[10], (TOKENS, INNER), 1.0, 6.0, ((0, 64), (1, 4)))
    step_raw = draw_step_raw(jax.random.fold_in(streams_of[16], 71), 0)
    decay_rate = draw_decay_rate(jax.random.fold_in(streams_of[16], 71), 0)
    skip_weight = jnp.clip(1.0 + 0.18 * jax.random.normal(streams_of[13], (HEADS,), jnp.float32), 0.1, 1.9)
    norm_gain = jnp.clip(1.0 + 0.18 * jax.random.normal(streams_of[14], (INNER,), jnp.float32), 0.1, 1.9)
    w_out = gaussian(streams_of[15], (D, INNER), INNER ** -0.5, 0.09375, ((1, 4),))
    return dict(moe_input=moe_input, cotangent=cotangent, expert_ids=expert_ids, routing_weights=routing_weights, gate_weight=gate_weight, up_weight=up_weight, down_weight=down_weight, inner_x=inner_x, inner_b=inner_b, inner_c=inner_c, gate_z=gate_z, step_raw=step_raw, decay_rate=decay_rate, skip_weight=skip_weight, norm_gain=norm_gain, w_out=w_out)


EPS = 0.01
HIGH = lax.Precision.HIGHEST

def slot_positions(chosen, expert_list, expert_capacity):
    listed = chosen.reshape(-1)
    onehot = (listed[:, None] == jnp.arange(expert_list, dtype=jnp.int32)[None, :]).astype(jnp.int32)
    before = jnp.cumsum(onehot, axis=0) - onehot
    return listed * expert_capacity + lax.optimization_barrier(jnp.sum(before * onehot, axis=1))

def prepare(inner_x32, inner_b32, step_raw, decays):
    tok_rows = inner_x32.shape[0]
    heads = decays.shape[0]
    groups = inner_b32.shape[1] // STATE
    per_group = heads // groups
    blocks = tok_rows // SPAN
    x_act = jax.nn.silu(inner_x32).reshape(tok_rows, heads, HEAD_DIM)
    b_blocks = jax.nn.silu(inner_b32).reshape(blocks, SPAN, groups, STATE)
    step_size = jax.nn.softplus(step_raw)
    decay_log = (-step_size * decays[None, :]).reshape(blocks, SPAN, groups, per_group)
    scaled = (x_act * step_size[:, :, None]).reshape(blocks, SPAN, groups, per_group, HEAD_DIM)
    return (x_act, b_blocks, decay_log, scaled)

def block_outputs(carry_state, block_in):
    x_block, log_block, b_block, c_block = block_in
    span_len = x_block.shape[0]
    running = jnp.cumsum(log_block, axis=0)
    places = jnp.arange(span_len)
    causal = (places[:, None] >= places[None, :])[:, :, None, None]
    between = running[:, None] - running[None, :]
    weights = jnp.where(causal, jnp.exp(jnp.where(causal, between, 0.0)), 0.0)
    scores = jnp.einsum('lgn,sgn->lsg', c_block, b_block, precision=HIGH)
    inside = jnp.einsum('lsg,lsge,sgep->lgep', scores, weights, x_block, precision=HIGH)
    carried = jnp.einsum('lgn,gepn,lge->lgep', c_block, carry_state, jnp.exp(running), precision=HIGH)
    to_end = jnp.exp(running[-1] - running)
    fresh_state = jnp.einsum('lgn,lge,lgep->gepn', b_block, to_end, x_block, precision=HIGH)
    return (carry_state * jnp.exp(running[-1])[:, :, None, None] + fresh_state, inside + carried)

def mixer_output(inner_x32, inner_b32, inner_c32, gate_z32, step_raw, carry_in, decays, skip_weight, norm_gain):
    tok_rows = inner_x32.shape[0]
    heads = decays.shape[0]
    groups = inner_b32.shape[1] // STATE
    x_act, b_blocks, decay_log, scaled = prepare(inner_x32, inner_b32, step_raw, decays)
    c_blocks = jax.nn.silu(inner_c32).reshape(tok_rows // SPAN, SPAN, groups, STATE)
    outputs = lax.scan(block_outputs, carry_in, (scaled, decay_log, b_blocks, c_blocks))[1]
    mixed_out = outputs.reshape(tok_rows, heads, HEAD_DIM) + x_act * skip_weight[None, :, None]
    gated_out = mixed_out.reshape(tok_rows, heads * HEAD_DIM) * jax.nn.silu(gate_z32)
    grouped = gated_out.reshape(tok_rows, groups, -1)
    normed = grouped * lax.rsqrt(lax.optimization_barrier(jnp.mean(grouped * grouped, axis=2, keepdims=True)) + EPS)
    return normed.reshape(tok_rows, -1) * norm_gain[None, :]

def expert_backward(padded_input, padded_gradient, item):
    owner, scaling, gate_w, up_w, down_w = item
    rows_in = padded_input[owner]
    rows_grad = (padded_gradient[owner].astype(jnp.float32) * scaling[:, None]).astype(jnp.bfloat16)
    gate_pre = jnp.dot(rows_in, gate_w, preferred_element_type=jnp.float32)
    up_pre = jnp.dot(rows_in, up_w, preferred_element_type=jnp.float32)
    sigmoid_gate = jax.nn.sigmoid(gate_pre)
    active = gate_pre * sigmoid_gate
    hidden = (active * up_pre).astype(jnp.bfloat16)
    hidden_grad = jnp.dot(rows_grad, down_w.T, preferred_element_type=jnp.float32)
    gate_grad = (hidden_grad * up_pre * sigmoid_gate * (1.0 + gate_pre * (1.0 - sigmoid_gate))).astype(jnp.bfloat16)
    up_grad = (hidden_grad * active).astype(jnp.bfloat16)
    down_part = jnp.dot(hidden.T, rows_grad, preferred_element_type=jnp.float32).astype(jnp.bfloat16)
    gate_part = jnp.dot(rows_in.T, gate_grad, preferred_element_type=jnp.float32).astype(jnp.bfloat16)
    up_part = jnp.dot(rows_in.T, up_grad, preferred_element_type=jnp.float32).astype(jnp.bfloat16)
    width = gate_w.shape[1] // N_TP
    summed = jnp.zeros(rows_in.shape, jnp.float32)
    for quarter in range(N_TP):
        low_col = quarter * width
        term = jnp.dot(gate_grad[:, low_col:low_col + width], gate_w[:, low_col:low_col + width].T, preferred_element_type=jnp.float32)
        term = term + jnp.dot(up_grad[:, low_col:low_col + width], up_w[:, low_col:low_col + width].T, preferred_element_type=jnp.float32)
        summed = summed + lax.optimization_barrier(term.astype(jnp.bfloat16)).astype(jnp.float32)
    return (gate_part, up_part, down_part, summed.astype(jnp.bfloat16))

def reference(moe_input, cotangent, expert_ids, routing_weights, gate_weight, up_weight, down_weight, inner_x, inner_b, inner_c, gate_z, step_raw, decay_rate, skip_weight, norm_gain, w_out):
    expert_list = gate_weight.shape[0]
    chosen_count = expert_ids.shape[1]
    expert_capacity = 4 * TOKENS_PER_SHARD // expert_list
    width = moe_input.shape[1]
    place_into_slots = jax.vmap(partial(slot_positions, expert_list=expert_list, expert_capacity=expert_capacity))(expert_ids.reshape(N_SP, TOKENS_PER_SHARD, chosen_count))
    local_owner = jnp.arange(TOKENS_PER_SHARD * chosen_count, dtype=jnp.int32) // chosen_count

    def routing_tables(spots, weights_block, block_index):
        owner = jnp.full((expert_list * expert_capacity,), TOKENS, jnp.int32).at[spots].set(local_owner + block_index * TOKENS_PER_SHARD)
        scaling = jnp.zeros((expert_list * expert_capacity,), jnp.float32).at[spots].set(weights_block)
        return (owner, scaling)
    owning_experts, scale_factors = jax.vmap(routing_tables)(place_into_slots, routing_weights.reshape(N_SP, TOKENS_PER_SHARD * chosen_count), jnp.arange(N_SP, dtype=jnp.int32))
    owning_experts = owning_experts.reshape(N_SP, expert_list, expert_capacity).transpose(1, 0, 2).reshape(expert_list, N_SP * expert_capacity)
    scale_factors = scale_factors.reshape(N_SP, expert_list, expert_capacity).transpose(1, 0, 2).reshape(expert_list, N_SP * expert_capacity)
    padded_input = jnp.concatenate([moe_input, jnp.zeros((1, width), jnp.bfloat16)], axis=0)
    padded_gradient = jnp.concatenate([cotangent, jnp.zeros((1, width), jnp.bfloat16)], axis=0)
    gate_weight_gradient, up_weight_gradient, down_weight_gradient, slot_gradient = lax.map(partial(expert_backward, padded_input, padded_gradient), (owning_experts, scale_factors, gate_weight, up_weight, down_weight))
    by_block = slot_gradient.reshape(expert_list, N_SP, expert_capacity, width).transpose(1, 0, 2, 3).reshape(N_SP, expert_list * expert_capacity, width)

    def collect(rows_block, spots):
        return rows_block[spots].astype(jnp.float32)
    moe_grad = lax.optimization_barrier(jnp.sum(jax.vmap(collect)(by_block, place_into_slots).reshape(TOKENS, chosen_count, width), axis=1))
    mixer_grad = (cotangent.astype(jnp.float32) + moe_grad).astype(jnp.bfloat16)
    groups = inner_b.shape[1] // STATE
    per_group = decay_rate.shape[0] // groups
    zero_state = jnp.zeros((groups, per_group, HEAD_DIM, STATE), jnp.float32)

    def forward(x_in, b_in, c_in, z_in, raw_in):
        return mixer_output(x_in, b_in, c_in, z_in, raw_in, zero_state, decay_rate, skip_weight, norm_gain)
    normed, pullback = jax.vjp(forward, inner_x.astype(jnp.float32), inner_b.astype(jnp.float32), inner_c.astype(jnp.float32), gate_z.astype(jnp.float32), step_raw)
    norm_out = normed.astype(jnp.bfloat16)
    grad_out = jnp.dot(mixer_grad.T, norm_out, preferred_element_type=jnp.float32)
    norm_grad = jnp.dot(mixer_grad, w_out, preferred_element_type=jnp.float32)
    x_grad, b_grad, c_grad, z_grad, raw_grad = pullback(norm_grad)
    return (gate_weight_gradient, up_weight_gradient, down_weight_gradient, grad_out, x_grad.astype(jnp.bfloat16), b_grad, c_grad, z_grad.astype(jnp.bfloat16), raw_grad)
```

```python
import jax
import jax.numpy as jnp
from jax import lax
from jax.experimental import pallas as pl
from jax.experimental.pallas import tpu as pltpu
from jax.sharding import Mesh
from jax.sharding import PartitionSpec as P

SP = ("sp_0", "sp_1", "sp_2")

NZ, NY, NC, NX = 8, 4, 2, 4
PEERS = 64
DIMS_TN = (((0,), (0,)), ((), ()))
DIMS_NT = (((1,), (1,)), ((), ()))
DIMS_NN = (((1,), (0,)), ((), ()))
F32 = jnp.float32
BF16 = jnp.bfloat16
MESH = pl.DeviceIdType.MESH


def mm(a, b, dims=DIMS_NN):
    return lax.dot_general(a, b, dims, preferred_element_type=F32)


def plane_at(z, i):
    odd = lax.rem(i, 2)
    off = odd * lax.div(i + 1, 2) + (1 - odd) * (NZ - lax.div(i, 2))
    return lax.rem(z + off, NZ)


def tok_slots(ids):
    e_iota = lax.broadcasted_iota(jnp.int32, (PEERS, 128), 0)
    hot = [(jnp.broadcast_to(ids[k : k + 1, :], (PEERS, 128)) == e_iota).astype(F32) for k in (0, 1)]
    earlier = (
        lax.broadcasted_iota(jnp.int32, (128, 128), 0) < lax.broadcasted_iota(jnp.int32, (128, 128), 1)
    ).astype(BF16)
    counts = mm((hot[0] + hot[1]).astype(BF16), earlier)
    return [
        ids[k : k + 1, :].astype(F32) * 8.0 + jnp.sum(hot[k] * counts, axis=0, keepdims=True)
        for k in (0, 1)
    ]


def to_column(row):
    eye = lax.broadcasted_iota(jnp.int32, (128, 128), 0) == lax.broadcasted_iota(
        jnp.int32, (128, 128), 1
    )
    return jnp.sum(jnp.where(eye, jnp.broadcast_to(row, (128, 128)), 0.0), axis=1, keepdims=True)


EPS = 0.01


def split2(v):
    hi = v.astype(BF16)
    return hi, (v - hi.astype(F32)).astype(BF16)


def spread(v, e):
    hi, lo = split2(v)
    return mm(hi, e) + mm(lo, e)


def per_head(v, e):
    hi, lo = split2(v)
    return mm(hi, e, DIMS_NT) + mm(lo, e, DIMS_NT)


def tri_sum(tri, v):
    hi = v.astype(BF16)
    rest = v - hi.astype(F32)
    mid = rest.astype(BF16)
    lo = (rest - mid.astype(F32)).astype(BF16)
    return mm(tri, hi) + mm(tri, mid) + mm(tri, lo)


def sigmoid(v):
    return 1.0 / (1.0 + jnp.exp(-v))


def iota(shape, dim):
    return lax.broadcasted_iota(jnp.int32, shape, dim)


def head_map():
    return (lax.div(iota((16, 1024), 1), 64) == iota((16, 1024), 0)).astype(F32).astype(BF16)


def two_rows(dec):
    hi = dec.astype(BF16).astype(F32)
    row = iota((16, dec.shape[1]), 0)
    return jnp.where(row == 0, hi, jnp.where(row == 1, dec - hi, 0.0))


def fused_kernel(
    ids_ref, wts_ref, min_ref, cot_ref, ix_ref, ib_ref, ic_ref, gz_ref, raw_ref, decay_ref,
    skip_ref, gain_ref, gw_hbm, uw_hbm, dw_hbm, wo_hbm,
    go_ref, gx_ref, gb_ref, gc_ref, gzz_ref, graw_ref, gwg_hbm, uwg_hbm, dwg_hbm,
    sendbuf, ybuf, gw, uw, dw, own_acc, nbr_acc, rs1_s, rs1_r, rs2_s, rs2_r,
    ggi, hid, retbuf, backbuf, rows, gout, dout,
    w_sem, o_sem, disp_ss, disp_rs, ret_ss, ret_rs,
    a1_s, a1_r, a2_s, a2_r, r1_s, r1_r, r2_s, r2_r, m_s, m_r,
    wo, scaled_ref, stepx_ref, erx_ref, tex_ref, r_ref, rt_ref, scores_ref, w_ref, m_ref,
    inside_ref, carry_ref, carried_ref, nr, gated_ref, inv_ref, dy_ref, ds1_ref, dsc_ref,
    msg_a, rec_a, msg_b, rec_b, msg_c, rec_c, pref, prefd, turned, turned_in, part, parts_in,
    sa_s, sa_r, sb_s, sb_r, sc_s, sc_r, n_s, n_r, t1_s, t1_r, t2_s, t2_r,
):
    z, y, c, x = (lax.axis_index(a) for a in ("sp_0", "sp_1", "sp_2", "tp"))
    sp = z * 8 + y * 2 + c
    me_yc = y * 2 + c
    right, left = lax.rem(x + 1, NX), lax.rem(x + 3, NX)
    far = lax.rem(x + 2, NX)

    def peer(zz, m):
        return {"sp_0": zz, "sp_1": lax.div(m, 2), "sp_2": lax.rem(m, 2)}

    barrier = pltpu.get_barrier_semaphore()

    def greet(i, carry):
        zz, m = lax.div(i, 8), lax.rem(i, 8)

        @pl.when(i != sp)
        def _():
            pl.semaphore_signal(barrier, inc=1, device_id=peer(zz, m), device_id_type=MESH)

        return carry

    lax.fori_loop(0, PEERS, greet, 0)
    for side in (right, left):
        pl.semaphore_signal(barrier, inc=1, device_id={"tp": side}, device_id_type=MESH)

    loads = [
        pltpu.make_async_copy(src, dst, w_sem.at[k])
        for k, (src, dst) in enumerate(((gw_hbm, gw), (uw_hbm, uw), (dw_hbm, dw), (wo_hbm, wo)))
    ]
    for load in loads:
        load.start()

    ids = ids_ref[...]
    wts = wts_ref[...]
    place = tok_slots(ids)
    tokens_in = min_ref[...]
    tokens_gr = cot_ref[...]

    def build(i, carry):
        base = (i * 64).astype(F32)
        slot = base + lax.broadcasted_iota(jnp.int32, (64, 128), 0).astype(F32)
        hits = [slot == jnp.broadcast_to(place[k], (64, 128)) for k in (0, 1)]
        pick = (hits[0] | hits[1]).astype(F32)
        weight = jnp.sum(
            jnp.where(hits[0], jnp.broadcast_to(wts[0:1, :], (64, 128)), 0.0)
            + jnp.where(hits[1], jnp.broadcast_to(wts[1:2, :], (64, 128)), 0.0),
            axis=1, keepdims=True,
        )
        pick = pick.astype(BF16)
        part_in = mm(pick, tokens_in).reshape(8, 8, 512)
        part_gr = (mm(pick, tokens_gr) * weight).reshape(8, 8, 512)
        sendbuf[pl.ds(i * 8, 8)] = jnp.concatenate([part_in, part_gr], axis=1).astype(BF16)
        return carry

    lax.fori_loop(0, 8, build, 0)
    ybuf[x, sp] = sendbuf[sp]

    pl.semaphore_wait(barrier, PEERS - 1 + 2)

    def dispatch(i, carry):
        zz = plane_at(z, lax.div(i, 8))
        m = lax.rem(me_yc + lax.rem(i, 8), 8)

        @pl.when(i != 0)
        def _():
            pltpu.make_async_remote_copy(
                src_ref=sendbuf.at[zz * 8 + m], dst_ref=ybuf.at[x, sp],
                send_sem=disp_ss.at[zz], recv_sem=disp_rs.at[z],
                device_id=peer(zz, m), device_id_type=MESH,
            ).start()

        return carry

    lax.fori_loop(0, PEERS, dispatch, 0)

    def plane_copy(buf, count, zz, ssem, rsem):
        return pltpu.make_async_remote_copy(
            src_ref=buf.at[pl.ds(zz * 8, count)], dst_ref=buf.at[pl.ds(zz * 8, count)],
            send_sem=ssem.at[zz], recv_sem=rsem.at[zz],
            device_id={"tp": right}, device_id_type=MESH,
        )

    def to_side(d, src, dst, ssem, rsem, k):
        return pltpu.make_async_remote_copy(
            src_ref=src, dst_ref=dst, send_sem=ssem.at[d, k], recv_sem=rsem.at[d, k],
            device_id={"tp": right if d == 0 else left}, device_id_type=MESH,
        )

    def a1(d, zz):
        blk = ybuf.at[x, pl.ds(zz * 8, 8)]
        return to_side(d, blk, blk, a1_s, a1_r, zz)

    def a2(d, zz):
        blk = ybuf.at[left if d == 0 else right, pl.ds(zz * 8 + 4 * d, 4)]
        return to_side(d, blk, blk, a2_s, a2_r, zz)

    def r1(d, zz):
        return to_side(d, rs1_s.at[d, zz], rs1_r.at[d, zz], r1_s, r1_r, zz)

    def r2(d, zz):
        return to_side(d, rs2_s.at[d, zz], rs2_r.at[d, zz], r2_s, r2_r, zz)


    def group_send(buf, land, m, ssem, rsem):
        return pltpu.make_async_remote_copy(
            src_ref=buf.at[m], dst_ref=land.at[me_yc], send_sem=ssem, recv_sem=rsem,
            device_id=peer(z, m), device_id_type=MESH,
        )

    def plane_send(src, land, zz, ssem, rsem):
        return pltpu.make_async_remote_copy(
            src_ref=src, dst_ref=land.at[z], send_sem=ssem, recv_sem=rsem,
            device_id=peer(zz, me_yc), device_id_type=MESH,
        )

    def seven(buf, ssem, rsem):
        blk = buf.at[pl.ds(0, 7)]
        return pltpu.make_async_remote_copy(
            src_ref=blk, dst_ref=blk, send_sem=ssem, recv_sem=rsem,
            device_id={"tp": right}, device_id_type=MESH,
        )

    def scan_a(k, state, dec):
        full = jnp.concatenate([state, two_rows(dec)], axis=0).astype(BF16)
        for j in range(8):
            msg_a[k, j] = full[:, j * 128 : (j + 1) * 128]
        rec_a[k, me_yc] = msg_a[k, me_yc]

        def go(t, carry):
            m = lax.rem(me_yc + t, 8)
            group_send(msg_a.at[k], rec_a.at[k], m, sa_s.at[k], sa_r.at[k]).start()
            return carry

        lax.fori_loop(1, 8, go, 0)

    def scan_b(k, order):
        seven(rec_a.at[k], sa_s.at[k], sa_r.at[k]).wait_recv()
        state = jnp.zeros((64, 128), F32)
        dec = jnp.ones((1, 128), F32)
        for m in order:
            pref[k, m] = state
            prefd[k, m] = jnp.broadcast_to(dec, (8, 128))
            tail = rec_a[k, m, 64:80].astype(F32)
            own = tail[0:1] + tail[1:2]
            state = state * own + rec_a[k, m, 0:64].astype(F32)
            dec = dec * own
        msg_b[k] = jnp.concatenate([state, two_rows(dec)], axis=0).astype(BF16)
        rec_b[k, z] = msg_b[k]

        def go(t, carry):
            zz = lax.rem(z + t, NZ)
            plane_send(msg_b.at[k], rec_b.at[k], zz, sb_s.at[k], sb_r.at[k]).start()
            return carry

        lax.fori_loop(1, NZ, go, 0)

    def scan_c(k, order):
        seven(rec_b.at[k], sb_s.at[k], sb_r.at[k]).wait_recv()
        state = jnp.zeros((64, 128), F32)
        for zz in order:
            tail = rec_b[k, zz, 64:80].astype(F32)
            nxt = state * (tail[0:1] + tail[1:2]) + rec_b[k, zz, 0:64].astype(F32)
            passed = (zz < z) if order[0] == 0 else (zz > z)
            state = jnp.where(passed, nxt, state)
        for m in range(8):
            msg_c[k, m] = (state * prefd[k, m][0:1] + pref[k, m]).astype(BF16)
        rec_c[k, me_yc] = msg_c[k, me_yc]

        def go(t, carry):
            m = lax.rem(me_yc + t, 8)
            group_send(msg_c.at[k], rec_c.at[k], m, sc_s.at[k], sc_r.at[k]).start()
            return carry

        lax.fori_loop(1, 8, go, 0)

    def scan_d(k):
        seven(rec_c.at[k], sc_s.at[k], sc_r.at[k]).wait_recv()
        return jnp.concatenate([rec_c[k, j] for j in range(8)], axis=1)

    up_order = tuple(range(8))
    down_order = tuple(reversed(range(8)))

    def mix_prepare():
        e = head_map()
        raw = raw_ref[...]
        step_size = jnp.maximum(raw, 0.0) + jnp.log1p(jnp.exp(-jnp.abs(raw)))
        dlog = -step_size * decay_ref[...]
        tri = (iota((128, 128), 0) >= iota((128, 128), 1)).astype(F32).astype(BF16)
        running = tri_sum(tri, dlog)
        r_ref[...] = running
        padded = jnp.concatenate([running, jnp.zeros((128, 112), F32)], axis=1)
        rt_ref[...] = padded.T
        stepx = spread(step_size, e)
        stepx_ref[...] = stepx
        erx_ref[...] = spread(jnp.exp(running), e)
        tex = spread(jnp.exp(running[127:128] - running), e)
        tex_ref[...] = tex
        xin = ix_ref[...].astype(F32)
        scaled = xin * sigmoid(xin) * stepx
        scaled_ref[...] = scaled
        bin_ = ib_ref[...].astype(F32)
        cin = ic_ref[...].astype(F32)
        b_act = (bin_ * sigmoid(bin_)).astype(BF16)
        c_act = (cin * sigmoid(cin)).astype(BF16)
        scores_ref[...] = mm(c_act, b_act, DIMS_NT)
        fresh = mm(b_act, (scaled * tex).astype(BF16), DIMS_TN)
        scan_a(0, fresh, erx_ref[127:128, :])

    def pair_forward(p, carry):
        lanes = pl.ds(pl.multiple_of(p * 128, 128), 128)
        sc = scaled_ref[:, lanes]
        low = iota((128, 128), 1) < 64
        causal = iota((128, 128), 0) >= iota((128, 128), 1)
        rhs = jnp.concatenate(
            [jnp.where(low, sc, 0.0).astype(BF16), jnp.where(low, 0.0, sc).astype(BF16)], axis=0
        )
        running = r_ref[...]
        scores = scores_ref[...]
        ms = []
        for k in (0, 1):
            h = 2 * p + k
            col = jnp.sum(jnp.where(iota((128, 16), 1) == h, running, 0.0), axis=1, keepdims=True)
            row = rt_ref[pl.ds(h, 1), :]
            w = jnp.exp(jnp.where(causal, col - row, -1e30))
            w_ref[h] = w
            ms.append((scores * w).astype(BF16))
            m_ref[h] = ms[k]
        inside_ref[:, lanes] = mm(jnp.concatenate(ms, axis=1), rhs)
        return carry

    def skip_lanes():
        return spread(jnp.broadcast_to(skip_ref[...], (8, 16)), head_map())[0:1]

    def mix_norm():
        state = scan_d(0)
        carry_ref[...] = state
        cin = ic_ref[...].astype(F32)
        c_act = (cin * sigmoid(cin)).astype(BF16)
        carried = mm(c_act, state) * erx_ref[...]
        carried_ref[...] = carried
        xin = ix_ref[...].astype(F32)
        zin = gz_ref[...].astype(F32)
        mixed = inside_ref[...] + carried + xin * sigmoid(xin) * skip_lanes()
        gated = mixed * (zin * sigmoid(zin))
        inv = lax.rsqrt(jnp.mean(gated * gated, axis=1, keepdims=True) + EPS)
        gated_ref[...] = gated
        inv_ref[...] = jnp.broadcast_to(inv, (128, 128))
        nr[me_yc] = (gated * inv * gain_ref[...]).astype(BF16)

    def n1(t):
        dev = {"sp_2": 1 - c} if t == 0 else {"sp_1": lax.rem(y + t, NY)}
        blk = nr.at[me_yc]
        return pltpu.make_async_remote_copy(
            src_ref=blk, dst_ref=blk, send_sem=n_s.at[t], recv_sem=n_r.at[t],
            device_id=dev, device_id_type=MESH,
        )

    def n2(t):
        blk = nr.at[lax.rem(y + NY - t, NY) * 2 + c]
        return pltpu.make_async_remote_copy(
            src_ref=blk, dst_ref=blk, send_sem=n_s.at[3 + t], recv_sem=n_r.at[3 + t],
            device_id={"sp_2": 1 - c}, device_id_type=MESH,
        )

    def step(i, carry):
        @pl.when(i < 8)
        def _():
            zz = plane_at(z, i)

            @pl.when(i == 0)
            def _():
                plane_copy(ybuf.at[x], 7, z, disp_ss, disp_rs).wait_recv()

            @pl.when(i > 0)
            def _():
                plane_copy(ybuf.at[x], 8, zz, disp_ss, disp_rs).wait_recv()

            a1(0, zz).start()
            a1(1, zz).start()

        @pl.when((i >= 1) & (i < 9))
        def _():
            zz = plane_at(z, i - 1)
            a1(0, zz).wait_recv()
            a2(0, zz).start()
            a1(1, zz).wait_recv()
            a2(1, zz).start()

        @pl.when((i >= 2) & (i < 10))
        def _():
            zz = plane_at(z, i - 2)
            a2(0, zz).wait_recv()
            a2(1, zz).wait_recv()

            @pl.when(i == 2)
            def _():
                for load in loads[:3]:
                    load.wait()

            gate = jnp.zeros((128, 256), F32)
            up = jnp.zeros((128, 256), F32)
            hgrad = jnp.zeros((128, 256), F32)
            for q in range(NX):
                rowsq = ybuf[q, pl.ds(zz * 8, 8)].reshape(128, 512)
                gate += mm(rowsq, gw[q])
                up += mm(rowsq, uw[q])
                hgrad += mm(rowsq, dw[:, q * 512 : (q + 1) * 512], DIMS_NT)
            gate = gate.reshape(8, 16, 256)[:, :8]
            up = up.reshape(8, 16, 256)[:, :8]
            hgrad = hgrad.reshape(8, 16, 256)[:, 8:]
            sig = 1.0 / (1.0 + jnp.exp(-gate))
            act = gate * sig
            zero = jnp.zeros((8, 8, 256), F32)
            hid[pl.ds(zz * 8, 8)] = jnp.concatenate([zero, act * up], axis=1).astype(BF16)
            gg = hgrad * up * sig * (1.0 + gate * (1.0 - sig))
            ug = hgrad * act
            ggi[pl.ds(zz * 8, 8), :, 0:256] = jnp.concatenate([gg, zero], axis=1).astype(BF16)
            ggi[pl.ds(zz * 8, 8), :, 256:512] = jnp.concatenate([ug, zero], axis=1).astype(BF16)
            ggc = gg.reshape(64, 256).astype(BF16)
            ugc = ug.reshape(64, 256).astype(BF16)

            def terms(q):
                return mm(ggc, gw[q], DIMS_NT) + mm(ugc, uw[q], DIMS_NT)

            away = terms(far).astype(BF16)
            rs1_s[0, zz] = away[:32]
            rs1_s[1, zz] = away[32:]
            r1(0, zz).start()
            r1(1, zz).start()
            nbr_acc[0, zz] = terms(right)
            nbr_acc[1, zz] = terms(left)
            own_acc[zz] = terms(x)

        @pl.when((i >= 3) & (i < 11))
        def _():
            zz = plane_at(z, i - 3)
            r1(0, zz).wait_recv()
            rs2_s[0, zz, 0:32] = (nbr_acc[0, zz, 0:32] + rs1_r[0, zz].astype(F32)).astype(BF16)
            rs2_s[0, zz, 32:64] = nbr_acc[0, zz, 32:64].astype(BF16)
            r2(0, zz).start()
            r1(1, zz).wait_recv()
            rs2_s[1, zz, 0:32] = nbr_acc[1, zz, 0:32].astype(BF16)
            rs2_s[1, zz, 32:64] = (nbr_acc[1, zz, 32:64] + rs1_r[1, zz].astype(F32)).astype(BF16)
            r2(1, zz).start()

        @pl.when(i >= 4)
        def _():
            zz = plane_at(z, i - 4)
            r2(0, zz).wait_recv()
            r2(1, zz).wait_recv()
            total = own_acc[zz] + rs2_r[0, zz].astype(F32) + rs2_r[1, zz].astype(F32)
            total = total.reshape(8, 8, 512)
            retbuf[pl.ds(zz * 8, 8)] = jnp.concatenate(
                [total[:, :, :256], total[:, :, 256:]], axis=1
            ).astype(BF16)

            @pl.when(i == 4)
            def _():
                backbuf[sp] = retbuf[sp]

            def give(k, inner):
                m = lax.rem(me_yc + k, 8)

                @pl.when((k > 0) | (i > 4))
                def _():
                    pltpu.make_async_remote_copy(
                        src_ref=retbuf.at[zz * 8 + m], dst_ref=backbuf.at[sp],
                        send_sem=ret_ss.at[zz], recv_sem=ret_rs.at[z],
                        device_id=peer(zz, m), device_id_type=MESH,
                    ).start()

                return inner

            lax.fori_loop(0, 8, give, 0)

        @pl.when(i == 0)
        def _():
            mix_prepare()

        @pl.when(i == 2)
        def _():
            scan_b(0, up_order)

        @pl.when((i >= 3) & (i < 7))
        def _():
            pair_forward(2 * (i - 3), 0)
            pair_forward(2 * (i - 3) + 1, 0)

        @pl.when(i == 4)
        def _():
            scan_c(0, up_order)

        @pl.when(i == 7)
        def _():
            mix_norm()
            for t in range(4):
                n1(t).start()

        @pl.when(i == 10)
        def _():
            for t in range(1, 4):
                n1(t).wait_recv()
                n2(t).start()

        return carry

    lax.fori_loop(0, 12, step, 0)

    def weights_in(q):
        g = mm(ybuf[q].reshape(1024, 512), ggi[...].reshape(1024, 512), DIMS_TN)
        gout[0, q] = g[:, :256].astype(BF16)
        gout[1, q] = g[:, 256:].astype(BF16)

    def weights_down(q):
        d = mm(hid[...].reshape(1024, 256), ybuf[q].reshape(1024, 512), DIMS_TN)
        dout[:, q * 512 : (q + 1) * 512] = d.astype(BF16)

    weights_in(0)
    weights_in(1)

    def arrive(k, carry):
        zz = plane_at(z, k)

        @pl.when(k == 0)
        def _():
            plane_copy(backbuf, 7, z, ret_ss, ret_rs).wait_recv()

        @pl.when(k > 0)
        def _():
            plane_copy(backbuf, 8, zz, ret_ss, ret_rs).wait_recv()

        return carry

    lax.fori_loop(0, NZ, arrive, 0)
    r_iota = lax.broadcasted_iota(jnp.int32, (128, 1024), 1)
    slot_of = ((r_iota // 16) * 8 + r_iota % 8).astype(F32)
    upper = (r_iota % 16) >= 8
    hit = (slot_of == to_column(place[0])) | (slot_of == to_column(place[1]))
    low = (hit & jnp.logical_not(upper)).astype(F32).astype(BF16)
    high = (hit & upper).astype(F32).astype(BF16)
    back = backbuf[...].reshape(1024, 256)
    moe_grad = jnp.concatenate([mm(low, back), mm(high, back)], axis=1)
    rows[x] = (tokens_gr.astype(F32) + moe_grad).astype(BF16)

    def m1(d):
        return to_side(d, rows.at[x], rows.at[x], m_s, m_r, 0)

    def m2(d):
        blk = rows.at[left if d == 0 else right, pl.ds(64 * d, 64)]
        return to_side(d, blk, blk, m_s, m_r, 1)

    m1(0).start()
    m1(1).start()
    weights_in(2)
    m1(0).wait_recv()
    m2(0).start()
    m1(1).wait_recv()
    m2(1).start()
    weights_in(3)
    m2(0).wait_recv()
    m2(1).wait_recv()

    for q in range(NX):
        turned[2 * q : 2 * q + 2] = rows[q].T.reshape(2, 8, 32, 128)
    turned_in[me_yc] = turned[:, me_yc]

    def t1(m):
        return pltpu.make_async_remote_copy(
            src_ref=turned.at[:, m], dst_ref=turned_in.at[me_yc],
            send_sem=t1_s.at[0], recv_sem=t1_r.at[0],
            device_id=peer(z, m), device_id_type=MESH,
        )

    def t1_go(t, carry):
        t1(lax.rem(me_yc + t, 8)).start()
        return carry

    lax.fori_loop(1, 8, t1_go, 0)

    loads[3].wait()
    norm_grad = mm(rows[0], wo[0])
    for q in range(1, NX):
        norm_grad += mm(rows[q], wo[q])
    inv = inv_ref[:, 0:1]
    gated = gated_ref[...]
    scale = norm_grad * gain_ref[...]
    dgated = scale * inv - gated * (inv * inv * inv * jnp.mean(gated * scale, axis=1, keepdims=True))
    zin = gz_ref[...].astype(F32)
    zsig = sigmoid(zin)
    dmix = dgated * (zin * zsig)
    dy_ref[...] = dmix
    cin = ic_ref[...].astype(F32)
    c_sig = sigmoid(cin)
    c_act = (cin * c_sig).astype(BF16)
    leaving = (dmix * erx_ref[...]).astype(BF16)
    scan_a(1, mm(c_act, leaving, DIMS_TN), erx_ref[127:128, :])
    xin = ix_ref[...].astype(F32)
    xsig = sigmoid(xin)
    mixed = inside_ref[...] + carried_ref[...] + xin * xsig * skip_lanes()
    gzz_ref[...] = (dgated * mixed * (zsig * (1.0 + zin * (1.0 - zsig)))).astype(BF16)
    dsc_ref[...] = jnp.zeros((128, 128), F32)

    def pair_back(p, carry):
        lanes = pl.ds(pl.multiple_of(p * 128, 128), 128)
        dy = dy_ref[:, lanes]
        low = iota((128, 128), 1) < 64
        both = jnp.concatenate(
            [jnp.where(low, dy, 0.0).astype(BF16), jnp.where(low, 0.0, dy).astype(BF16)], axis=0
        )
        ds1_ref[:, lanes] = mm(m_ref[pl.ds(2 * p, 2)].reshape(256, 128), both, DIMS_TN)
        dm = mm(both, scaled_ref[:, lanes].astype(BF16), DIMS_NT)
        dsc_ref[...] += dm[:128] * w_ref[2 * p] + dm[128:] * w_ref[2 * p + 1]
        return carry

    lax.fori_loop(0, 4, pair_back, 0)
    scan_b(1, down_order)
    n1(0).wait_recv()
    for t in range(1, 4):
        n2(t).wait_recv()
    seven(turned_in, t1_s.at[0], t1_r.at[0]).wait_recv()
    terms_out = mm(turned_in[0].reshape(256, 128), nr[0])
    for m in range(1, 8):
        terms_out += mm(turned_in[m].reshape(256, 128), nr[m])
    part[...] = terms_out.reshape(8, 32, 1024).astype(BF16)
    parts_in[z] = part[z]

    def t2_go(t, carry):
        zz = lax.rem(z + t, NZ)
        plane_send(part.at[zz], parts_in, zz, t2_s.at[0], t2_r.at[0]).start()
        return carry

    lax.fori_loop(1, NZ, t2_go, 0)
    lax.fori_loop(4, 8, pair_back, 0)
    scan_c(1, down_order)
    state = carry_ref[...]
    dsc = dsc_ref[...].astype(BF16)
    bin_ = ib_ref[...].astype(F32)
    b_sig = sigmoid(bin_)
    b_act = (bin_ * b_sig).astype(BF16)
    dc = mm(dsc, b_act) + mm(leaving, state, DIMS_NT)
    gc_ref[...] = dc * (c_sig * (1.0 + cin * (1.0 - c_sig)))
    e = head_map()
    dmix_b = dmix.astype(BF16).astype(F32)
    scaled = scaled_ref[...]
    scaled_b = scaled.astype(BF16).astype(F32)
    ds1 = ds1_ref[...]
    turn = per_head(dmix_b * inside_ref[...] + dmix * carried_ref[...] - scaled_b * ds1, e)
    for q in range(2):
        weights_down(q)
    after = scan_d(1)
    tex = tex_ref[...]
    ds2 = mm(b_act, after) * tex
    db = mm(dsc, c_act, DIMS_TN) + mm((scaled * tex).astype(BF16), after, DIMS_NT)
    gb_ref[...] = db * (b_sig * (1.0 + bin_ * (1.0 - b_sig)))
    dscaled = ds1 + ds2
    gx_ref[...] = (
        (dscaled * stepx_ref[...] + dmix * skip_lanes()) * (xsig * (1.0 + xin * (1.0 - xsig)))
    ).astype(BF16)
    fade = per_head(scaled * ds2, e)
    at_end = jnp.sum(after.astype(F32) * state.astype(F32), axis=0, keepdims=True)
    at_end = per_head(jnp.broadcast_to(at_end, (8, 1024)), e)[0:1]
    at_end = jnp.sum(fade, axis=0, keepdims=True) + at_end * jnp.exp(r_ref[127:128, :])
    later = (iota((128, 128), 0) <= iota((128, 128), 1)).astype(F32).astype(BF16)
    dlog_grad = tri_sum(later, turn - fade) + at_end
    raw = raw_ref[...]
    dstep = per_head(dscaled * (xin * xsig), e) - dlog_grad * decay_ref[...]
    graw_ref[...] = dstep * sigmoid(raw)
    for q in range(2, NX):
        weights_down(q)
    outs = [
        pltpu.make_async_copy(src, dst, o_sem.at[k])
        for k, (src, dst) in enumerate(((gout.at[0], gwg_hbm), (gout.at[1], uwg_hbm), (dout, dwg_hbm)))
    ]
    for out in outs:
        out.start()
    seven(parts_in, t2_s.at[0], t2_r.at[0]).wait_recv()
    total = parts_in[0].astype(F32)
    for zz in range(1, NZ):
        total += parts_in[zz].astype(F32)
    go_ref[...] = total

    def drain(k, carry):
        @pl.when(k == z)
        def _():
            plane_copy(sendbuf, 7, k, disp_ss, disp_rs).wait_send()
            plane_copy(retbuf, 7, k, ret_ss, ret_rs).wait_send()

        @pl.when(k != z)
        def _():
            plane_copy(sendbuf, 8, k, disp_ss, disp_rs).wait_send()
            plane_copy(retbuf, 8, k, ret_ss, ret_rs).wait_send()

        for d in (0, 1):
            a1(d, k).wait_send()
            a2(d, k).wait_send()
            r1(d, k).wait_send()
            r2(d, k).wait_send()
        return carry

    lax.fori_loop(0, NZ, drain, 0)
    for d in (0, 1):
        m1(d).wait_send()
        m2(d).wait_send()
    for k in (0, 1):
        seven(msg_a.at[k], sa_s.at[k], sa_r.at[k]).wait_send()
        seven(rec_b.at[k], sb_s.at[k], sb_r.at[k]).wait_send()
        seven(msg_c.at[k], sc_s.at[k], sc_r.at[k]).wait_send()
    for t in range(4):
        n1(t).wait_send()
    for t in range(1, 4):
        n2(t).wait_send()
    seven(turned_in, t1_s.at[0], t1_r.at[0]).wait_send()
    seven(part, t2_s.at[0], t2_r.at[0]).wait_send()
    for out in outs:
        out.wait()


def fused_call(
    moe_input, cotangent, expert_ids, routing_weights, gate_weight, up_weight, down_weight,
    inner_x, inner_b, inner_c, gate_z, step_raw, decay_rate, skip_weight, norm_gain, w_out,
):
    vmem = pl.BlockSpec(memory_space=pltpu.VMEM)
    hbm = pl.BlockSpec(memory_space=pl.ANY)
    dma = pltpu.SemaphoreType.DMA
    V = pltpu.VMEM
    S = jax.ShapeDtypeStruct
    sems = [dma((4,)), dma((3,)), dma((8,)), dma((8,)), dma((8,)), dma((8,))]
    sems += [dma((2, 8))] * 8 + [dma((2, 2))] * 2
    wide = V((128, 1024), F32)
    go, gx, gb, gc, gzz, graw, gwg, uwg, dwg = pl.pallas_call(
        fused_kernel,
        name="fused",
        out_shape=(
            S((32, 1024), F32), S((128, 1024), BF16), S((128, 64), F32), S((128, 64), F32),
            S((128, 1024), BF16), S((128, 16), F32),
            S((NX, 512, 256), BF16), S((NX, 512, 256), BF16), S((256, 2048), BF16),
        ),
        in_specs=[vmem] * 12 + [hbm] * 4,
        out_specs=(vmem,) * 6 + (hbm,) * 3,
        scratch_shapes=[
            V((64, 16, 512), BF16), V((NX, 64, 16, 512), BF16),
            V((NX, 512, 256), BF16), V((NX, 512, 256), BF16), V((256, 2048), BF16),
            V((8, 64, 512), F32), V((2, 8, 64, 512), F32),
            V((2, 8, 32, 512), BF16), V((2, 8, 32, 512), BF16),
            V((2, 8, 64, 512), BF16), V((2, 8, 64, 512), BF16),
            V((64, 16, 512), BF16), V((64, 16, 256), BF16),
            V((64, 16, 256), BF16), V((64, 16, 256), BF16),
            V((NX, 128, 512), BF16), V((2, NX, 512, 256), BF16), V((256, 2048), BF16),
        ] + sems + [
            V((NX, 512, 1024), BF16), wide, wide, wide, wide, V((128, 16), F32),
            V((128, 128), F32), V((128, 128), F32), V((16, 128, 128), F32),
            V((16, 128, 128), BF16), wide, V((64, 1024), BF16), wide,
            V((8, 128, 1024), BF16), wide, V((128, 128), F32), wide, wide, V((128, 128), F32),
            V((2, 8, 80, 128), BF16), V((2, 8, 80, 128), BF16), V((2, 80, 128), BF16),
            V((2, 8, 80, 128), BF16), V((2, 8, 64, 128), BF16), V((2, 8, 64, 128), BF16),
            V((2, 8, 64, 128), F32), V((2, 8, 8, 128), F32),
            V((8, 8, 32, 128), BF16), V((8, 8, 32, 128), BF16),
            V((8, 32, 1024), BF16), V((8, 32, 1024), BF16),
        ] + [dma((2,))] * 6 + [dma((7,))] * 2 + [dma((1,))] * 4,
        compiler_params=pltpu.CompilerParams(
            collective_id=0, has_side_effects=True, vmem_limit_bytes=63 * 1024 * 1024
        ),
    )(
        expert_ids.T, routing_weights.T, moe_input, cotangent,
        inner_x, inner_b, inner_c, gate_z, step_raw,
        decay_rate.reshape(1, 16), skip_weight.reshape(1, 16), norm_gain.reshape(1, 1024),
        gate_weight.reshape(NX, 512, 256), up_weight.reshape(NX, 512, 256),
        down_weight.reshape(256, 2048), w_out.reshape(NX, 512, 1024),
    )
    return (
        gwg.reshape(1, 2048, 256), uwg.reshape(1, 2048, 256), dwg.reshape(1, 256, 2048),
        go, gx, gb, gc, gzz, graw,
    )


def solution(mesh):
    finer = Mesh(mesh.devices.reshape(8, 4, 2, mesh.shape["tp"]), ("sp_0", "sp_1", "sp_2", "tp"))
    return jax.shard_map(
        fused_call,
        mesh=finer,
        in_specs=(
            P(SP, "tp"),
            P(SP, "tp"),
            P(SP, None),
            P(SP, None),
            P(SP, None, "tp"),
            P(SP, None, "tp"),
            P(SP, "tp", None),
            P(SP, "tp"),
            P(SP, "tp"),
            P(SP, "tp"),
            P(SP, "tp"),
            P(SP, "tp"),
            P("tp"),
            P("tp"),
            P("tp"),
            P(None, "tp"),
        ),
        out_specs=(
            P(SP, None, "tp"),
            P(SP, None, "tp"),
            P(SP, "tp", None),
            P(SP, "tp"),
            P(SP, "tp"),
            P(SP, "tp"),
            P(SP, "tp"),
            P(SP, "tp"),
            P(SP, "tp"),
        ),
        check_vma=False,
    )
```

```python
import jax
import jax.numpy as jnp
from jax import lax
from jax.experimental import pallas as pl
from jax.experimental.pallas import tpu as pltpu
from jax.sharding import Mesh
from jax.sharding import PartitionSpec as P

SP = ("sp_0", "sp_1", "sp_2")

NZ, NY, NC, NX = 8, 4, 2, 4
PEERS = 64
DIMS_TN = (((0,), (0,)), ((), ()))
DIMS_NT = (((1,), (1,)), ((), ()))
DIMS_NN = (((1,), (0,)), ((), ()))
F32 = jnp.float32
BF16 = jnp.bfloat16
MESH = pl.DeviceIdType.MESH


def mm(a, b, dims=DIMS_NN):
    return lax.dot_general(a, b, dims, preferred_element_type=F32)


def offset_at(i):
    off = jnp.int32(0)
    for k, at in enumerate((0, 1, 7, 2, 6, 4, 3, 5)):
        off = jnp.where(i == k, at, off)
    return off


def plane_at(z, i):
    return lax.rem(z + offset_at(i), NZ)


def tok_slots(ids):
    e_iota = lax.broadcasted_iota(jnp.int32, (PEERS, 128), 0)
    hot = [(jnp.broadcast_to(ids[k : k + 1, :], (PEERS, 128)) == e_iota).astype(F32) for k in (0, 1)]
    earlier = (
        lax.broadcasted_iota(jnp.int32, (128, 128), 0) < lax.broadcasted_iota(jnp.int32, (128, 128), 1)
    ).astype(BF16)
    counts = mm((hot[0] + hot[1]).astype(BF16), earlier)
    return [
        ids[k : k + 1, :].astype(F32) * 8.0 + jnp.sum(hot[k] * counts, axis=0, keepdims=True)
        for k in (0, 1)
    ]


def to_column(row):
    eye = lax.broadcasted_iota(jnp.int32, (128, 128), 0) == lax.broadcasted_iota(
        jnp.int32, (128, 128), 1
    )
    return jnp.sum(jnp.where(eye, jnp.broadcast_to(row, (128, 128)), 0.0), axis=1, keepdims=True)


EPS = 0.01


def split2(v):
    hi = v.astype(BF16)
    return hi, (v - hi.astype(F32)).astype(BF16)


def spread(v, e):
    hi, lo = split2(v)
    return mm(hi, e) + mm(lo, e)


def per_head(v, e):
    hi, lo = split2(v)
    return mm(hi, e, DIMS_NT) + mm(lo, e, DIMS_NT)


def tri_sum(tri, v):
    hi = v.astype(BF16)
    rest = v - hi.astype(F32)
    mid = rest.astype(BF16)
    lo = (rest - mid.astype(F32)).astype(BF16)
    return mm(tri, hi) + mm(tri, mid) + mm(tri, lo)


def sigmoid(v):
    return 1.0 / (1.0 + jnp.exp(-v))


def iota(shape, dim):
    return lax.broadcasted_iota(jnp.int32, shape, dim)


def head_map():
    return (lax.div(iota((16, 1024), 1), 64) == iota((16, 1024), 0)).astype(F32).astype(BF16)


def upright(narrow):
    return jnp.concatenate([narrow, jnp.zeros((112, 128), F32)], axis=0).T[:, 0:16]


def flat(narrow):
    return jnp.concatenate([narrow, jnp.zeros((128, 112), F32)], axis=1).T[0:16]


def two_rows(dec):
    hi = dec.astype(BF16).astype(F32)
    row = iota((16, dec.shape[1]), 0)
    return jnp.where(row == 0, hi, jnp.where(row == 1, dec - hi, 0.0))


def fused_kernel(
    ids_hbm, wts_hbm, min_hbm, cot_hbm, ix_hbm, ib_hbm, ic_hbm, gz_hbm, raw_hbm, decay_hbm,
    skip_hbm, gain_hbm, gw_hbm, uw_hbm, dw_hbm, wo_hbm,
    go_hbm, gx_hbm, gb_hbm, gc_hbm, gzz_hbm, graw_hbm, gwg_hbm, uwg_hbm, dwg_hbm,
    sendbuf, ybuf, gw, uw, dw, own_acc, nbr_acc, rs1_s, rs1_r, rs2_s, rs2_r,
    ggi, hid, retbuf, backbuf, rows, gout, dout,
    w_sem, o_sem, disp_ss, disp_rs, ret_ss, ret_rs,
    a1_s, a1_r, a2_s, a2_r, r1_s, r1_r, r2_s, r2_r, m_s, m_r,
    go_ref, gx_ref, gb_ref, gc_ref, gzz_ref, graw_ref, bmsg_a, brec_a, bmsg_b, brec_b,
    carried_back, far_in, bb_s, bb_r, t3_s, t3_r,
    ids_ref, wts_ref, min_ref, cot_ref, ix_ref, ib_ref, ic_ref, gz_ref, raw_ref, decay_ref,
    skip_ref, gain_ref, wo, scaled_ref, stepx_ref, erx_ref, tex_ref, r_ref, rt_ref, scores_ref, w_ref, m_ref,
    inside_ref, carry_ref, carried_ref, nr, gated_ref, inv_ref, dy_ref, ds1_ref, dsc_ref,
    msg_a, rec_a, msg_b, rec_b, msg_c, rec_c, pref, prefd, turned, tin, part, parts_in,
    sa_s, sa_r, sb_s, sb_r, sc_s, sc_r, n_s, n_r, t1_s, t1_r, t2_s, t2_r, u_s, u_r,
):
    z, y, c, x = (lax.axis_index(a) for a in ("sp_0", "sp_1", "sp_2", "tp"))
    sp = z * 8 + y * 2 + c
    me_yc = y * 2 + c
    right, left = lax.rem(x + 1, NX), lax.rem(x + 3, NX)
    far = lax.rem(x + 2, NX)

    def peer(zz, m):
        return {"sp_0": zz, "sp_1": lax.div(m, 2), "sp_2": lax.rem(m, 2)}

    barrier = pltpu.get_barrier_semaphore()

    loads = [
        pltpu.make_async_copy(src, dst, w_sem.at[k])
        for k, (src, dst) in enumerate((
            (ids_hbm, ids_ref), (wts_hbm, wts_ref), (min_hbm, min_ref), (cot_hbm, cot_ref),
            (ix_hbm, ix_ref), (ib_hbm, ib_ref), (ic_hbm, ic_ref), (gz_hbm, gz_ref),
            (raw_hbm, raw_ref), (decay_hbm, decay_ref), (skip_hbm, skip_ref), (gain_hbm, gain_ref),
            (gw_hbm, gw), (uw_hbm, uw), (dw_hbm, dw), (wo_hbm, wo),
        ))
    ]
    for load in loads[:4]:
        load.start()

    def greet(i, carry):
        zz, m = lax.div(i, 8), lax.rem(i, 8)

        @pl.when(i != sp)
        def _():
            pl.semaphore_signal(barrier, inc=1, device_id=peer(zz, m), device_id_type=MESH)

        return carry

    lax.fori_loop(0, PEERS, greet, 0)
    for side in (right, left):
        pl.semaphore_signal(barrier, inc=1, device_id={"tp": side}, device_id_type=MESH)

    for load in loads[4:]:
        load.start()
    for load in loads[:4]:
        load.wait()

    ids = ids_ref[...]
    wts = wts_ref[...]
    place = tok_slots(ids)
    tokens_in = min_ref[...]
    tokens_gr = cot_ref[...]

    def build(i, carry):
        base = (i * 64).astype(F32)
        slot = base + lax.broadcasted_iota(jnp.int32, (64, 128), 0).astype(F32)
        hits = [slot == jnp.broadcast_to(place[k], (64, 128)) for k in (0, 1)]
        pick = (hits[0] | hits[1]).astype(F32)
        weight = jnp.sum(
            jnp.where(hits[0], jnp.broadcast_to(wts[0:1, :], (64, 128)), 0.0)
            + jnp.where(hits[1], jnp.broadcast_to(wts[1:2, :], (64, 128)), 0.0),
            axis=1, keepdims=True,
        )
        pick = pick.astype(BF16)
        part_in = mm(pick, tokens_in).reshape(8, 8, 512)
        part_gr = (mm(pick, tokens_gr) * weight).reshape(8, 8, 512)
        sendbuf[pl.ds(i * 8, 8)] = jnp.concatenate([part_in, part_gr], axis=1).astype(BF16)
        return carry

    lax.fori_loop(0, 8, build, 0)
    ybuf[x, sp] = sendbuf[sp]

    pl.semaphore_wait(barrier, PEERS - 1 + 2)

    def dispatch(i, carry):
        zz = lax.rem(z + NZ - offset_at(lax.div(i, 8)), NZ)
        m = lax.rem(me_yc + lax.rem(i, 8), 8)

        @pl.when(i != 0)
        def _():
            pltpu.make_async_remote_copy(
                src_ref=sendbuf.at[zz * 8 + m], dst_ref=ybuf.at[x, sp],
                send_sem=disp_ss.at[0], recv_sem=disp_rs.at[z],
                device_id=peer(zz, m), device_id_type=MESH,
            ).start()

        return carry

    lax.fori_loop(0, 8, dispatch, 0)

    def waiter(blk, ssem, rsem):
        return pltpu.make_async_remote_copy(
            src_ref=blk, dst_ref=blk, send_sem=ssem, recv_sem=rsem,
            device_id={"tp": right}, device_id_type=MESH,
        )

    def plane_copy(buf, count, zz, ssem, rsem):
        return waiter(buf.at[pl.ds(zz * 8, count)], ssem.at[0], rsem.at[zz])

    def to_side(d, src, dst, ssem, rsem):
        return pltpu.make_async_remote_copy(
            src_ref=src, dst_ref=dst, send_sem=ssem, recv_sem=rsem,
            device_id={"tp": right if d == 0 else left}, device_id_type=MESH,
        )

    def a1(d, zz):
        blk = ybuf.at[x, pl.ds(zz * 8, 8)]
        return to_side(d, blk, blk, a1_s.at[0], a1_r.at[d, zz])

    def a2(d, zz):
        blk = ybuf.at[left if d == 0 else right, pl.ds(zz * 8 + 4 * d, 4)]
        return to_side(d, blk, blk, a2_s.at[0], a2_r.at[zz])

    def r1(d, zz):
        return to_side(d, rs1_s.at[d, zz], rs1_r.at[d, zz], r1_s.at[0], r1_r.at[d, zz])

    def r2(d, zz):
        return to_side(d, rs2_s.at[d, zz], rs2_r.at[d, zz], r2_s.at[0], r2_r.at[zz])


    def group_send(buf, land, m, ssem, rsem):
        return pltpu.make_async_remote_copy(
            src_ref=buf.at[m], dst_ref=land.at[me_yc], send_sem=ssem, recv_sem=rsem,
            device_id=peer(z, m), device_id_type=MESH,
        )

    def plane_send(src, land, zz, ssem, rsem):
        return pltpu.make_async_remote_copy(
            src_ref=src, dst_ref=land.at[z], send_sem=ssem, recv_sem=rsem,
            device_id=peer(zz, me_yc), device_id_type=MESH,
        )

    def seven(buf, ssem, rsem):
        blk = buf.at[pl.ds(0, 7)]
        return pltpu.make_async_remote_copy(
            src_ref=blk, dst_ref=blk, send_sem=ssem, recv_sem=rsem,
            device_id={"tp": right}, device_id_type=MESH,
        )

    def scan_a(state, dec):
        full = jnp.concatenate([state, two_rows(dec)], axis=0).astype(BF16)
        for j in range(8):
            msg_a[j] = full[:, j * 128 : (j + 1) * 128]
        rec_a[me_yc] = msg_a[me_yc]

        def go(t, carry):
            m = lax.rem(me_yc + t, 8)
            group_send(msg_a, rec_a, m, sa_s.at[0], sa_r.at[0]).start()
            return carry

        lax.fori_loop(1, 8, go, 0)

    def scan_b():
        seven(rec_a, sa_s.at[0], sa_r.at[0]).wait_recv()
        state = jnp.zeros((64, 128), F32)
        dec = jnp.ones((1, 128), F32)
        for m in up_order:
            pref[m] = state
            prefd[m] = jnp.broadcast_to(dec, (8, 128))
            tail = rec_a[m, 64:80].astype(F32)
            own = tail[0:1] + tail[1:2]
            state = state * own + rec_a[m, 0:64].astype(F32)
            dec = dec * own
        msg_b[...] = jnp.concatenate([state, two_rows(dec)], axis=0).astype(BF16)
        rec_b[z] = msg_b[...]

        def go(t, carry):
            zz = lax.rem(z + t, NZ)
            plane_send(msg_b, rec_b, zz, sb_s.at[0], sb_r.at[0]).start()
            return carry

        lax.fori_loop(1, NZ, go, 0)

    def scan_c():
        seven(rec_b, sb_s.at[0], sb_r.at[0]).wait_recv()
        state = jnp.zeros((64, 128), F32)
        for zz in up_order:
            tail = rec_b[zz, 64:80].astype(F32)
            nxt = state * (tail[0:1] + tail[1:2]) + rec_b[zz, 0:64].astype(F32)
            state = jnp.where(zz < z, nxt, state)
        for m in range(8):
            msg_c[0, m] = (state * prefd[m][0:1] + pref[m]).astype(BF16)
        rec_c[0, me_yc] = msg_c[0, me_yc]

        def go(t, carry):
            m = lax.rem(me_yc + t, 8)
            group_send(msg_c.at[0], rec_c.at[0], m, sc_s.at[0], sc_r.at[0]).start()
            return carry

        lax.fori_loop(1, 8, go, 0)

    def scan_d(k):
        seven(rec_c.at[k], sc_s.at[k], sc_r.at[k]).wait_recv()
        return jnp.concatenate([rec_c[k, j] for j in range(8)], axis=1)

    up_order = tuple(range(8))
    down_order = tuple(reversed(range(8)))

    def decay_row(tail):
        tail = tail.astype(F32)
        return tail[0:1] + tail[1:2]

    def back_a(state):
        full = state.astype(BF16)
        for j in range(8):
            bmsg_a[j] = full[:, j * 128 : (j + 1) * 128]
        brec_a[me_yc] = bmsg_a[me_yc]

        def go(t, carry):
            m = lax.rem(me_yc + t, 8)
            group_send(bmsg_a, brec_a, m, sa_s.at[1], sa_r.at[1]).start()
            return carry

        lax.fori_loop(1, 8, go, 0)

    def back_send(zz):
        return pltpu.make_async_remote_copy(
            src_ref=bmsg_b, dst_ref=brec_b.at[z], send_sem=bb_s.at[zz], recv_sem=bb_r.at[z],
            device_id=peer(zz, me_yc), device_id_type=MESH,
        )

    def back_recv(zz):
        return pltpu.make_async_remote_copy(
            src_ref=bmsg_b, dst_ref=brec_b.at[zz], send_sem=bb_s.at[zz], recv_sem=bb_r.at[zz],
            device_id={"tp": right}, device_id_type=MESH,
        )

    def back_b():
        seven(brec_a, sa_s.at[1], sa_r.at[1]).wait_recv()
        state = jnp.zeros((64, 128), F32)
        dec = jnp.ones((1, 128), F32)
        for m in down_order:
            pref[m] = state
            prefd[m] = jnp.broadcast_to(dec, (8, 128))
            own = decay_row(rec_a[m, 64:80])
            state = state * own + brec_a[m].astype(F32)
            dec = dec * own
        bmsg_b[...] = state.astype(BF16)
        for zz in down_order:

            @pl.when(zz < z)
            def _():
                back_send(zz).start()

    def back_c():
        carried_back[...] = jnp.zeros((64, 128), F32)
        for zz in down_order[:-1]:

            @pl.when(zz > z)
            def _():
                back_recv(zz).wait_recv()
                carried_back[...] = carried_back[...] * decay_row(rec_b[zz, 64:80]) + brec_b[
                    zz
                ].astype(F32)

        state = carried_back[...]
        for m in range(8):
            msg_c[1, m] = (state * prefd[m][0:1] + pref[m]).astype(BF16)
        rec_c[1, me_yc] = msg_c[1, me_yc]

        def go(t, carry):
            m = lax.rem(me_yc + t, 8)
            group_send(msg_c.at[1], rec_c.at[1], m, sc_s.at[1], sc_r.at[1]).start()
            return carry

        lax.fori_loop(1, 8, go, 0)

    def mix_prepare():
        for load in loads[4:12]:
            load.wait()
        e = head_map()
        raw = upright(raw_ref[...])
        step_size = jnp.maximum(raw, 0.0) + jnp.log1p(jnp.exp(-jnp.abs(raw)))
        dlog = -step_size * decay_ref[...]
        tri = (iota((128, 128), 0) >= iota((128, 128), 1)).astype(F32).astype(BF16)
        running = tri_sum(tri, dlog)
        r_ref[...] = running
        rt_ref[...] = flat(running)
        stepx = spread(step_size, e)
        stepx_ref[...] = stepx
        erx_ref[...] = spread(jnp.exp(running), e)
        tex = spread(jnp.exp(running[127:128] - running), e)
        tex_ref[...] = tex
        xin = ix_ref[...].astype(F32)
        scaled = xin * sigmoid(xin) * stepx
        scaled_ref[...] = scaled
        bin_ = ib_ref[...].astype(F32).T
        cin = ic_ref[...].astype(F32).T
        b_act = (bin_ * sigmoid(bin_)).astype(BF16)
        c_act = (cin * sigmoid(cin)).astype(BF16)
        scores_ref[...] = mm(c_act, b_act, DIMS_NT)
        fresh = mm(b_act, (scaled * tex).astype(BF16), DIMS_TN)
        scan_a(fresh, erx_ref[127:128, :])

    def pair_forward(p, carry):
        lanes = pl.ds(pl.multiple_of(p * 128, 128), 128)
        sc = scaled_ref[:, lanes]
        low = iota((128, 128), 1) < 64
        causal = iota((128, 128), 0) >= iota((128, 128), 1)
        rhs = jnp.concatenate(
            [jnp.where(low, sc, 0.0).astype(BF16), jnp.where(low, 0.0, sc).astype(BF16)], axis=0
        )
        running = r_ref[...]
        scores = scores_ref[...]
        ms = []
        for k in (0, 1):
            h = 2 * p + k
            col = jnp.sum(jnp.where(iota((128, 16), 1) == h, running, 0.0), axis=1, keepdims=True)
            row = rt_ref[pl.ds(h, 1), :]
            w = jnp.exp(jnp.where(causal, col - row, -1e30))
            w_ref[h] = w
            ms.append((scores * w).astype(BF16))
            m_ref[h] = ms[k]
        inside_ref[:, lanes] = mm(jnp.concatenate(ms, axis=1), rhs)
        return carry

    def skip_lanes():
        return spread(jnp.broadcast_to(skip_ref[...], (8, 16)), head_map())[0:1]

    def mix_norm():
        state = scan_d(0)
        carry_ref[...] = state
        cin = ic_ref[...].astype(F32).T
        c_act = (cin * sigmoid(cin)).astype(BF16)
        carried = mm(c_act, state) * erx_ref[...]
        carried_ref[...] = carried
        xin = ix_ref[...].astype(F32)
        zin = gz_ref[...].astype(F32)
        mixed = inside_ref[...] + carried + xin * sigmoid(xin) * skip_lanes()
        gated = mixed * (zin * sigmoid(zin))
        inv = lax.rsqrt(jnp.mean(gated * gated, axis=1, keepdims=True) + EPS)
        gated_ref[...] = gated
        inv_ref[...] = jnp.broadcast_to(inv, (128, 128))
        nr[me_yc] = (gated * inv * gain_ref[...]).astype(BF16)

    def n1(t):
        dev = {"sp_2": 1 - c} if t == 0 else {"sp_1": lax.rem(y + t, NY)}
        blk = nr.at[me_yc]
        return pltpu.make_async_remote_copy(
            src_ref=blk, dst_ref=blk, send_sem=n_s.at[t], recv_sem=n_r.at[t],
            device_id=dev, device_id_type=MESH,
        )

    def n2(t):
        blk = nr.at[lax.rem(y + NY - t, NY) * 2 + c]
        return pltpu.make_async_remote_copy(
            src_ref=blk, dst_ref=blk, send_sem=n_s.at[3 + t], recv_sem=n_r.at[3 + t],
            device_id={"sp_2": 1 - c}, device_id_type=MESH,
        )

    def step(i, carry):
        def take_plane():
            zz = plane_at(z, i)

            @pl.when(i == 0)
            def _():
                plane_copy(ybuf.at[x], 7, z, disp_ss, disp_rs).wait_recv()

            @pl.when(i > 0)
            def _():
                plane_copy(ybuf.at[x], 8, zz, disp_ss, disp_rs).wait_recv()

            a1(0, zz).start()
            a1(1, zz).start()

            @pl.when(i < 2)
            def _():
                lax.fori_loop(16 * i + 8, 16 * i + 24, dispatch, 0)

            @pl.when(i == 2)
            def _():
                lax.fori_loop(40, 48, dispatch, 0)

            @pl.when(i == 3)
            def _():
                lax.fori_loop(48, PEERS, dispatch, 0)

        pl.when((i < 8) & (i != 1))(take_plane)

        @pl.when((i >= 1) & (i < 9))
        def _():
            zz = plane_at(z, i - 1)
            a1(0, zz).wait_recv()
            a2(0, zz).start()
            a1(1, zz).wait_recv()
            a2(1, zz).start()

        pl.when(i == 1)(take_plane)

        @pl.when((i >= 2) & (i < 10))
        def _():
            zz = plane_at(z, i - 2)

            @pl.when(i == 2)
            def _():
                for load in loads[12:15]:
                    load.wait()

            gate = jnp.zeros((128, 256), F32)
            up = jnp.zeros((128, 256), F32)
            hgrad = jnp.zeros((128, 256), F32)
            for q in (x, left, right, far):
                if q is far:
                    waiter(ybuf.at[far, pl.ds(zz * 8, 8)], a2_s.at[0], a2_r.at[zz]).wait_recv()
                rowsq = ybuf[q, pl.ds(zz * 8, 8)].reshape(128, 512)
                gate += mm(rowsq, gw[q])
                up += mm(rowsq, uw[q])
                hgrad += mm(
                    rowsq, dw[:, pl.ds(pl.multiple_of(q * 512, 512), 512)], DIMS_NT
                )
            gate = gate.reshape(8, 16, 256)[:, :8]
            up = up.reshape(8, 16, 256)[:, :8]
            hgrad = hgrad.reshape(8, 16, 256)[:, 8:]
            sig = 1.0 / (1.0 + jnp.exp(-gate))
            act = gate * sig
            zero = jnp.zeros((8, 8, 256), F32)
            hid[pl.ds(zz * 8, 8)] = jnp.concatenate([zero, act * up], axis=1).astype(BF16)
            gg = hgrad * up * sig * (1.0 + gate * (1.0 - sig))
            ug = hgrad * act
            ggi[pl.ds(zz * 8, 8), :, 0:256] = jnp.concatenate([gg, zero], axis=1).astype(BF16)
            ggi[pl.ds(zz * 8, 8), :, 256:512] = jnp.concatenate([ug, zero], axis=1).astype(BF16)
            ggc = gg.reshape(64, 256).astype(BF16)
            ugc = ug.reshape(64, 256).astype(BF16)

            def terms(q):
                return mm(ggc, gw[q], DIMS_NT) + mm(ugc, uw[q], DIMS_NT)

            away = terms(far).astype(BF16)
            rs1_s[0, zz] = away[:32]
            rs1_s[1, zz] = away[32:]
            r1(0, zz).start()
            r1(1, zz).start()
            nbr_acc[0, zz] = terms(right)
            nbr_acc[1, zz] = terms(left)
            own_acc[zz] = terms(x)

        @pl.when((i >= 3) & (i < 11))
        def _():
            zz = plane_at(z, i - 3)
            r1(0, zz).wait_recv()
            rs2_s[0, zz, 0:32] = (nbr_acc[0, zz, 0:32] + rs1_r[0, zz].astype(F32)).astype(BF16)
            rs2_s[0, zz, 32:64] = nbr_acc[0, zz, 32:64].astype(BF16)
            r2(0, zz).start()
            r1(1, zz).wait_recv()
            rs2_s[1, zz, 0:32] = nbr_acc[1, zz, 0:32].astype(BF16)
            rs2_s[1, zz, 32:64] = (nbr_acc[1, zz, 32:64] + rs1_r[1, zz].astype(F32)).astype(BF16)
            r2(1, zz).start()

        @pl.when(i >= 4)
        def _():
            zz = plane_at(z, i - 4)
            waiter(rs2_r.at[:, zz], r2_s.at[0], r2_r.at[zz]).wait_recv()
            total = own_acc[zz] + rs2_r[0, zz].astype(F32) + rs2_r[1, zz].astype(F32)
            total = total.reshape(8, 8, 512)
            retbuf[pl.ds(zz * 8, 8)] = jnp.concatenate(
                [total[:, :, :256], total[:, :, 256:]], axis=1
            ).astype(BF16)

            @pl.when(i == 4)
            def _():
                backbuf[sp] = retbuf[sp]

            def give(k, inner):
                m = lax.rem(me_yc + k, 8)

                @pl.when((k > 0) | (i > 4))
                def _():
                    pltpu.make_async_remote_copy(
                        src_ref=retbuf.at[zz * 8 + m], dst_ref=backbuf.at[sp],
                        send_sem=ret_ss.at[0], recv_sem=ret_rs.at[z],
                        device_id=peer(zz, m), device_id_type=MESH,
                    ).start()

                return inner

            lax.fori_loop(0, 8, give, 0)

        @pl.when(i == 0)
        def _():
            mix_prepare()

        @pl.when(i == 2)
        def _():
            scan_b()

        @pl.when((i >= 3) & (i < 7))
        def _():
            pair_forward(2 * (i - 3), 0)
            pair_forward(2 * (i - 3) + 1, 0)

        @pl.when(i == 4)
        def _():
            scan_c()

        @pl.when(i == 7)
        def _():
            mix_norm()
            for t in range(4):
                n1(t).start()

        return carry

    lax.fori_loop(0, 12, step, 0)

    outs = [
        pltpu.make_async_copy(src, dst, o_sem.at[k])
        for k, (src, dst) in enumerate((
            (gout.at[0], gwg_hbm), (gout.at[1], uwg_hbm), (dout, dwg_hbm), (go_ref, go_hbm),
            (gx_ref, gx_hbm), (gb_ref, gb_hbm), (graw_ref, graw_hbm), (gc_ref, gc_hbm),
            (gzz_ref, gzz_hbm),
        ))
    ]

    def weights_in(q):
        g = mm(ybuf[q].reshape(1024, 512), ggi[...].reshape(1024, 512), DIMS_TN)
        gout[0, q] = g[:, :256].astype(BF16)
        gout[1, q] = g[:, 256:].astype(BF16)

    def weights_down(q):
        d = mm(hid[...].reshape(1024, 256), ybuf[q].reshape(1024, 512), DIMS_TN)
        dout[:, q * 512 : (q + 1) * 512] = d.astype(BF16)

    weights_in(0)
    weights_in(1)
    for t in range(1, 4):
        n1(t).wait_recv()
        n2(t).start()
    weights_in(2)
    weights_in(3)
    outs[0].start()
    outs[1].start()

    def arrive(k, carry):
        zz = plane_at(z, k)

        @pl.when(k == 0)
        def _():
            plane_copy(backbuf, 7, z, ret_ss, ret_rs).wait_recv()

        @pl.when(k > 0)
        def _():
            plane_copy(backbuf, 8, zz, ret_ss, ret_rs).wait_recv()

        return carry

    lax.fori_loop(0, NZ, arrive, 0)
    r_iota = lax.broadcasted_iota(jnp.int32, (128, 1024), 1)
    slot_of = ((r_iota // 16) * 8 + r_iota % 8).astype(F32)
    upper = (r_iota % 16) >= 8
    hit = (slot_of == to_column(place[0])) | (slot_of == to_column(place[1]))
    low = (hit & jnp.logical_not(upper)).astype(F32).astype(BF16)
    high = (hit & upper).astype(F32).astype(BF16)
    back = backbuf[...].reshape(1024, 256)
    moe_grad = jnp.concatenate([mm(low, back), mm(high, back)], axis=1)
    rows[x] = (tokens_gr.astype(F32) + moe_grad).astype(BF16)

    def m1(d, half):
        blk = rows.at[x, pl.ds(64 * ((d + half) % 2), 64)]
        return to_side(d, blk, blk, m_s.at[d, half], m_r.at[d, half])

    def m2(d):
        blk = rows.at[left if d == 0 else right, pl.ds(64 * d, 64)]
        return to_side(d, blk, blk, m_s.at[d, 2], m_r.at[d, 2])

    for half in (0, 1):
        for d in (0, 1):
            m1(d, half).start()

    own_t = rows[x].T.reshape(2, 8, 32, 128)
    for j in range(8):
        turned[j] = own_t[:, j]
    tin[x, me_yc] = turned[me_yc]

    def t1_go(t, carry):
        m = lax.rem(me_yc + t, 8)
        group_send(turned, tin.at[x], m, t1_s.at[0], t1_r.at[0]).start()
        return carry

    lax.fori_loop(1, 8, t1_go, 0)

    def u1(d):
        return to_side(d, tin.at[x], tin.at[x], u_s.at[d, 0], u_r.at[d, 0])

    def u2(d):
        blk = tin.at[left if d == 0 else right, pl.ds(4 * d, 4)]
        return to_side(d, blk, blk, u_s.at[d, 1], u_r.at[d, 1])

    loads[15].wait()
    norm_grad = mm(rows[x], wo[x])
    for d in (0, 1):
        m1(d, 0).wait_recv()
        m2(d).start()
    seven(tin.at[x], t1_s.at[0], t1_r.at[0]).wait_recv()
    u1(0).start()
    u1(1).start()
    for d in (0, 1):
        m1(d, 1).wait_recv()
    norm_grad += mm(rows[left], wo[left])
    norm_grad += mm(rows[right], wo[right])
    m2(0).wait_recv()
    m2(1).wait_recv()
    norm_grad += mm(rows[far], wo[far])
    inv = inv_ref[:, 0:1]
    gated = gated_ref[...]
    scale = norm_grad * gain_ref[...]
    dgated = scale * inv - gated * (inv * inv * inv * jnp.mean(gated * scale, axis=1, keepdims=True))
    zin = gz_ref[...].astype(F32)
    zsig = sigmoid(zin)
    dmix = dgated * (zin * zsig)
    dy_ref[...] = dmix
    cin = ic_ref[...].astype(F32).T
    c_sig = sigmoid(cin)
    c_act = (cin * c_sig).astype(BF16)
    leaving = (dmix * erx_ref[...]).astype(BF16)
    back_a(mm(c_act, leaving, DIMS_TN))
    u1(0).wait_recv()
    u2(0).start()
    u1(1).wait_recv()
    u2(1).start()
    xin = ix_ref[...].astype(F32)
    xsig = sigmoid(xin)
    mixed = inside_ref[...] + carried_ref[...] + xin * xsig * skip_lanes()
    gzz_ref[...] = (dgated * mixed * (zsig * (1.0 + zin * (1.0 - zsig)))).astype(BF16)
    outs[8].start()
    dsc_ref[...] = jnp.zeros((128, 128), F32)

    def pair_back(p, carry):
        lanes = pl.ds(pl.multiple_of(p * 128, 128), 128)
        dy = dy_ref[:, lanes]
        low = iota((128, 128), 1) < 64
        both = jnp.concatenate(
            [jnp.where(low, dy, 0.0).astype(BF16), jnp.where(low, 0.0, dy).astype(BF16)], axis=0
        )
        ds1_ref[:, lanes] = mm(m_ref[pl.ds(2 * p, 2)].reshape(256, 128), both, DIMS_TN)
        dm = mm(both, scaled_ref[:, lanes].astype(BF16), DIMS_NT)
        dsc_ref[...] += dm[:128] * w_ref[2 * p] + dm[128:] * w_ref[2 * p + 1]
        return carry

    lax.fori_loop(0, 4, pair_back, 0)
    n1(0).wait_recv()
    for t in range(1, 4):
        n2(t).wait_recv()
    u2(0).wait_recv()
    u2(1).wait_recv()
    terms_out = mm(tin[:, 0].reshape(256, 128), nr[0])
    for m in range(1, 8):
        terms_out += mm(tin[:, m].reshape(256, 128), nr[m])
    part[...] = terms_out.reshape(8, 32, 1024).astype(BF16)
    back_b()

    def at_plane(t):
        return lax.rem(z + t + NZ, NZ)

    def t2_far(d):
        return pltpu.make_async_remote_copy(
            src_ref=part.at[at_plane(4), pl.ds(16 * d, 16)], dst_ref=far_in.at[d],
            send_sem=t3_s.at[d], recv_sem=t3_r.at[d],
            device_id=peer(at_plane(1 - 2 * d), me_yc), device_id_type=MESH,
        )

    def t2(t):
        zz = at_plane(t)
        return plane_send(part.at[zz], parts_in, zz, t2_s.at[0], t2_r.at[0])

    def six(buf, ssem, rsem):
        blk = buf.at[pl.ds(0, 6)]
        return pltpu.make_async_remote_copy(
            src_ref=blk, dst_ref=blk, send_sem=ssem, recv_sem=rsem,
            device_id={"tp": right}, device_id_type=MESH,
        )

    t2_far(0).start()
    t2_far(1).start()
    for t in (1, -1, 2, -2):
        t2(t).start()
    lax.fori_loop(4, 8, pair_back, 0)
    back_c()
    t2_far(0).wait_recv()
    over = at_plane(3)
    part[over, 0:16] = (part[over, 0:16].astype(F32) + far_in[0].astype(F32)).astype(BF16)
    t2(3).start()
    t2_far(1).wait_recv()
    under = at_plane(-3)
    part[under, 16:32] = (part[under, 16:32].astype(F32) + far_in[1].astype(F32)).astype(BF16)
    t2(-3).start()
    state = carry_ref[...]
    dsc = dsc_ref[...].astype(BF16)
    bin_ = ib_ref[...].astype(F32).T
    b_sig = sigmoid(bin_)
    b_act = (bin_ * b_sig).astype(BF16)
    dc = mm(dsc, b_act) + mm(leaving, state, DIMS_NT)
    gc_ref[...] = (dc * (c_sig * (1.0 + cin * (1.0 - c_sig)))).T
    outs[7].start()
    e = head_map()
    dmix_b = dmix.astype(BF16).astype(F32)
    scaled = scaled_ref[...]
    scaled_b = scaled.astype(BF16).astype(F32)
    ds1 = ds1_ref[...]
    turn = per_head(dmix_b * inside_ref[...] + dmix * carried_ref[...] - scaled_b * ds1, e)
    for q in range(NX):
        weights_down(q)
    outs[2].start()
    after = scan_d(1)
    tex = tex_ref[...]
    ds2 = mm(b_act, after) * tex
    db = mm(dsc, c_act, DIMS_TN) + mm((scaled * tex).astype(BF16), after, DIMS_NT)
    gb_ref[...] = (db * (b_sig * (1.0 + bin_ * (1.0 - b_sig)))).T
    dscaled = ds1 + ds2
    gx_ref[...] = (
        (dscaled * stepx_ref[...] + dmix * skip_lanes()) * (xsig * (1.0 + xin * (1.0 - xsig)))
    ).astype(BF16)
    fade = per_head(scaled * ds2, e)
    at_end = jnp.sum(after.astype(F32) * state.astype(F32), axis=0, keepdims=True)
    at_end = per_head(jnp.broadcast_to(at_end, (8, 1024)), e)[0:1]
    at_end = jnp.sum(fade, axis=0, keepdims=True) + at_end * jnp.exp(r_ref[127:128, :])
    later = (iota((128, 128), 0) <= iota((128, 128), 1)).astype(F32).astype(BF16)
    dlog_grad = tri_sum(later, turn - fade) + at_end
    raw = upright(raw_ref[...])
    dstep = per_head(dscaled * (xin * xsig), e) - dlog_grad * decay_ref[...]
    graw_ref[...] = flat(dstep * sigmoid(raw))
    for k in range(4, 7):
        outs[k].start()
    waiter(sendbuf.at[pl.ds(0, 63)], disp_ss.at[0], disp_rs.at[0]).wait_send()
    waiter(retbuf.at[pl.ds(0, 63)], ret_ss.at[0], ret_rs.at[0]).wait_send()
    waiter(ybuf.at[pl.ds(0, 2)], a1_s.at[0], a1_r.at[0, 0]).wait_send()
    waiter(ybuf.at[0], a2_s.at[0], a2_r.at[0]).wait_send()
    waiter(rs1_s, r1_s.at[0], r1_r.at[0, 0]).wait_send()
    waiter(rs2_s, r2_s.at[0], r2_r.at[0]).wait_send()
    for d in (0, 1):
        m1(d, 0).wait_send()
        m1(d, 1).wait_send()
        m2(d).wait_send()
        u1(d).wait_send()
        u2(d).wait_send()
    seven(msg_a, sa_s.at[0], sa_r.at[0]).wait_send()
    seven(rec_b, sb_s.at[0], sb_r.at[0]).wait_send()
    seven(msg_c.at[0], sc_s.at[0], sc_r.at[0]).wait_send()
    seven(bmsg_a, sa_s.at[1], sa_r.at[1]).wait_send()
    seven(msg_c.at[1], sc_s.at[1], sc_r.at[1]).wait_send()
    for zz in range(NZ - 1):

        @pl.when(zz < z)
        def _():
            back_send(zz).wait_send()

    for t in range(4):
        n1(t).wait_send()
    for t in range(1, 4):
        n2(t).wait_send()
    seven(turned, t1_s.at[0], t1_r.at[0]).wait_send()
    t2_far(0).wait_send()
    t2_far(1).wait_send()
    six(part, t2_s.at[0], t2_r.at[0]).wait_send()
    six(parts_in, t2_s.at[0], t2_r.at[0]).wait_recv()
    total = part[at_plane(0)].astype(F32)
    for t in (1, -1, 2, -2, 3, -3):
        total += parts_in[at_plane(t)].astype(F32)
    go_ref[...] = total
    outs[3].start()
    for out in outs:
        out.wait()


def fused_call(
    moe_input, cotangent, expert_ids, routing_weights, gate_weight, up_weight, down_weight,
    inner_x, inner_b, inner_c, gate_z, step_raw, decay_rate, skip_weight, norm_gain, w_out,
):
    hbm = pl.BlockSpec(memory_space=pl.ANY)
    dma = pltpu.SemaphoreType.DMA
    V = pltpu.VMEM
    S = jax.ShapeDtypeStruct
    sems = [dma((16,)), dma((9,)), dma((1,)), dma((8,)), dma((1,)), dma((8,))]
    one, each, pairs = dma((1,)), dma((8,)), dma((2, 8))
    sems += [one, pairs, one, each, one, pairs, one, each] + [dma((2, 3))] * 2
    wide = V((128, 1024), F32)
    go, gx, gb, gc, gzz, graw, gwg, uwg, dwg = pl.pallas_call(
        fused_kernel,
        name="fused",
        out_shape=(
            S((32, 1024), F32), S((128, 1024), BF16), S((64, 128), F32), S((64, 128), F32),
            S((128, 1024), BF16), S((16, 128), F32),
            S((NX, 512, 256), BF16), S((NX, 512, 256), BF16), S((256, 2048), BF16),
        ),
        in_specs=[hbm] * 16,
        out_specs=(hbm,) * 9,
        scratch_shapes=[
            V((64, 16, 512), BF16), V((NX, 64, 16, 512), BF16),
            V((NX, 512, 256), BF16), V((NX, 512, 256), BF16), V((256, 2048), BF16),
            V((8, 64, 512), F32), V((2, 8, 64, 512), F32),
            V((2, 8, 32, 512), BF16), V((2, 8, 32, 512), BF16),
            V((2, 8, 64, 512), BF16), V((2, 8, 64, 512), BF16),
            V((64, 16, 512), BF16), V((64, 16, 256), BF16),
            V((64, 16, 256), BF16), V((64, 16, 256), BF16),
            V((NX, 128, 512), BF16), V((2, NX, 512, 256), BF16), V((256, 2048), BF16),
        ] + sems + [
            V((32, 1024), F32), V((128, 1024), BF16), V((64, 128), F32), V((64, 128), F32),
            V((128, 1024), BF16), V((16, 128), F32),
            V((8, 64, 128), BF16), V((8, 64, 128), BF16), V((64, 128), BF16),
            V((8, 64, 128), BF16), V((64, 128), F32), V((2, 16, 1024), BF16),
            dma((8,)), dma((8,)), dma((2,)), dma((2,)),
            V((2, 128), jnp.int32), V((2, 128), F32), V((128, 512), BF16), V((128, 512), BF16),
            V((128, 1024), BF16), V((64, 128), BF16), V((64, 128), BF16), V((128, 1024), BF16),
            V((16, 128), F32), V((1, 16), F32), V((1, 16), F32), V((1, 1024), F32),
            V((NX, 512, 1024), BF16), wide, wide, wide, wide, V((128, 16), F32),
            V((16, 128), F32), V((128, 128), F32), V((16, 128, 128), F32),
            V((16, 128, 128), BF16), wide, V((64, 1024), BF16), wide,
            V((8, 128, 1024), BF16), wide, V((128, 128), F32), wide, wide, V((128, 128), F32),
            V((8, 80, 128), BF16), V((8, 80, 128), BF16), V((80, 128), BF16),
            V((8, 80, 128), BF16), V((2, 8, 64, 128), BF16), V((2, 8, 64, 128), BF16),
            V((8, 64, 128), F32), V((8, 8, 128), F32),
            V((8, 2, 32, 128), BF16), V((NX, 8, 2, 32, 128), BF16),
            V((8, 32, 1024), BF16), V((8, 32, 1024), BF16),
        ] + [dma((2,))] * 6 + [dma((7,))] * 2 + [dma((1,))] * 4 + [dma((2, 2))] * 2,
        compiler_params=pltpu.CompilerParams(
            collective_id=0, has_side_effects=True, vmem_limit_bytes=63 * 1024 * 1024
        ),
    )(
        expert_ids.T, routing_weights.T, moe_input, cotangent,
        inner_x, inner_b.T, inner_c.T, gate_z, step_raw.T,
        decay_rate.reshape(1, 16), skip_weight.reshape(1, 16), norm_gain.reshape(1, 1024),
        gate_weight.reshape(NX, 512, 256), up_weight.reshape(NX, 512, 256),
        down_weight.reshape(256, 2048), w_out.reshape(NX, 512, 1024),
    )
    gwg, uwg, dwg, go, gx, gb, gc, gzz, graw = handed_over(
        gwg.reshape(2048, 256), uwg.reshape(2048, 256), dwg, go, gx, gb, gc, gzz, graw
    )
    return gwg[None], uwg[None], dwg[None], go, gx, gb.T, gc.T, gzz, graw.T


def hand_over_kernel(*refs):
    count = (len(refs) - 2) // 3
    srcs, dsts, held = refs[:count], refs[count : 2 * count], refs[2 * count : 3 * count]
    in_sem, out_sem = refs[3 * count :]
    ins = [pltpu.make_async_copy(srcs[k], held[k], in_sem.at[k]) for k in range(count)]
    outs = [pltpu.make_async_copy(held[k], dsts[k], out_sem.at[k]) for k in range(count)]
    for k in range(count):
        ins[k].start()
    for k in range(count):
        ins[k].wait()
        outs[k].start()
    for k in range(count):
        outs[k].wait()


def handed_over(*arrays):
    hbm = pl.BlockSpec(memory_space=pl.ANY)
    count = len(arrays)
    return pl.pallas_call(
        hand_over_kernel,
        name="handover",
        out_shape=tuple(jax.ShapeDtypeStruct(a.shape, a.dtype) for a in arrays),
        in_specs=[hbm] * count,
        out_specs=(hbm,) * count,
        scratch_shapes=[pltpu.VMEM(a.shape, a.dtype) for a in arrays]
        + [pltpu.SemaphoreType.DMA((count,))] * 2,
        compiler_params=pltpu.CompilerParams(vmem_limit_bytes=60 * 1024 * 1024),
    )(*arrays)


def solution(mesh):
    finer = Mesh(mesh.devices.reshape(8, 4, 2, mesh.shape["tp"]), ("sp_0", "sp_1", "sp_2", "tp"))
    return jax.shard_map(
        fused_call,
        mesh=finer,
        in_specs=(
            P(SP, "tp"),
            P(SP, "tp"),
            P(SP, None),
            P(SP, None),
            P(SP, None, "tp"),
            P(SP, None, "tp"),
            P(SP, "tp", None),
            P(SP, "tp"),
            P(SP, "tp"),
            P(SP, "tp"),
            P(SP, "tp"),
            P(SP, "tp"),
            P("tp"),
            P("tp"),
            P("tp"),
            P(None, "tp"),
        ),
        out_specs=(
            P(SP, None, "tp"),
            P(SP, None, "tp"),
            P(SP, "tp", None),
            P(SP, "tp"),
            P(SP, "tp"),
            P(SP, "tp"),
            P(SP, "tp"),
            P(SP, "tp"),
            P(SP, "tp"),
        ),
        check_vma=False,
    )
```

```python
import jax
import jax.numpy as jnp
from jax import lax
from jax.experimental import pallas as pl
from jax.experimental.pallas import tpu as pltpu
from jax.sharding import Mesh
from jax.sharding import PartitionSpec as P

SP = ("sp_0", "sp_1", "sp_2")

NZ, NY, NC, NX = 8, 4, 2, 4
PEERS = 64
DIMS_TN = (((0,), (0,)), ((), ()))
DIMS_NT = (((1,), (1,)), ((), ()))
DIMS_NN = (((1,), (0,)), ((), ()))
F32 = jnp.float32
BF16 = jnp.bfloat16
MESH = pl.DeviceIdType.MESH


def mm(a, b, dims=DIMS_NN):
    return lax.dot_general(a, b, dims, preferred_element_type=F32)


def offset_at(i):
    off = jnp.int32(0)
    for k, at in enumerate((0, 1, 7, 2, 6, 4, 3, 5)):
        off = jnp.where(i == k, at, off)
    return off


def plane_at(z, i):
    return lax.rem(z + offset_at(i), NZ)


def tok_slots(ids):
    e_iota = lax.broadcasted_iota(jnp.int32, (PEERS, 128), 0)
    hot = [(jnp.broadcast_to(ids[k : k + 1, :], (PEERS, 128)) == e_iota).astype(F32) for k in (0, 1)]
    earlier = (
        lax.broadcasted_iota(jnp.int32, (128, 128), 0) < lax.broadcasted_iota(jnp.int32, (128, 128), 1)
    ).astype(BF16)
    counts = mm((hot[0] + hot[1]).astype(BF16), earlier)
    return [
        ids[k : k + 1, :].astype(F32) * 8.0 + jnp.sum(hot[k] * counts, axis=0, keepdims=True)
        for k in (0, 1)
    ]


def to_column(row):
    eye = lax.broadcasted_iota(jnp.int32, (128, 128), 0) == lax.broadcasted_iota(
        jnp.int32, (128, 128), 1
    )
    return jnp.sum(jnp.where(eye, jnp.broadcast_to(row, (128, 128)), 0.0), axis=1, keepdims=True)


EPS = 0.01


def split2(v):
    hi = v.astype(BF16)
    return hi, (v - hi.astype(F32)).astype(BF16)


def spread(v, e):
    hi, lo = split2(v)
    return mm(hi, e) + mm(lo, e)


def per_head(v, e):
    hi, lo = split2(v)
    return mm(hi, e, DIMS_NT) + mm(lo, e, DIMS_NT)


def tri_sum(tri, v):
    hi = v.astype(BF16)
    rest = v - hi.astype(F32)
    mid = rest.astype(BF16)
    lo = (rest - mid.astype(F32)).astype(BF16)
    return mm(tri, hi) + mm(tri, mid) + mm(tri, lo)


def sigmoid(v):
    return 1.0 / (1.0 + jnp.exp(-v))


def iota(shape, dim):
    return lax.broadcasted_iota(jnp.int32, shape, dim)


def head_map():
    return (lax.div(iota((16, 1024), 1), 64) == iota((16, 1024), 0)).astype(F32).astype(BF16)


def upright(narrow):
    return jnp.concatenate([narrow, jnp.zeros((112, 128), F32)], axis=0).T[:, 0:16]


def flat(narrow):
    return jnp.concatenate([narrow, jnp.zeros((128, 112), F32)], axis=1).T[0:16]


def two_rows(dec):
    hi = dec.astype(BF16).astype(F32)
    row = iota((16, dec.shape[1]), 0)
    return jnp.where(row == 0, hi, jnp.where(row == 1, dec - hi, 0.0))


def fused_kernel(
    ids_hbm, wts_hbm, min_hbm, cot_hbm, ix_hbm, ib_hbm, ic_hbm, gz_hbm, raw_hbm, decay_hbm,
    skip_hbm, gain_hbm, gw_hbm, uw_hbm, dw_hbm, wo_hbm,
    go_ref, gx_ref, gb_ref, gc_ref, gzz_ref, graw_ref, gwg_ref, uwg_ref, dout,
    sendbuf, ybuf, gw, uw, dw, own_acc, nbr_acc, rs1_s, rs1_r, rs2_s, rs2_r,
    ggi, hid, retbuf, backbuf, rows,
    w_sem, disp_ss, disp_rs, ret_ss, ret_rs,
    a1_s, a1_r, a2_s, a2_r, r1_s, r1_r, r2_s, r2_r, m_s, m_r,
    bmsg_a, brec_a, bmsg_b, brec_b,
    carried_back, far_in, bb_s, bb_r, t3_s, t3_r,
    ids_ref, wts_ref, min_ref, cot_ref, ix_ref, ib_ref, ic_ref, gz_ref, raw_ref, decay_ref,
    skip_ref, gain_ref, wo, scaled_ref, stepx_ref, erx_ref, tex_ref, r_ref, rt_ref, scores_ref, w_ref, m_ref,
    inside_ref, carry_ref, carried_ref, nr, gated_ref, inv_ref, dy_ref, ds1_ref, dsc_ref,
    msg_a, rec_a, msg_b, rec_b, msg_c, rec_c, pref, prefd, turned, tin, part, parts_in,
    sa_s, sa_r, sb_s, sb_r, sc_s, sc_r, n_s, n_r, t1_s, t1_r, t2_s, t2_r, u_s, u_r,
):
    z, y, c, x = (lax.axis_index(a) for a in ("sp_0", "sp_1", "sp_2", "tp"))
    sp = z * 8 + y * 2 + c
    me_yc = y * 2 + c
    right, left = lax.rem(x + 1, NX), lax.rem(x + 3, NX)
    far = lax.rem(x + 2, NX)

    def peer(zz, m):
        return {"sp_0": zz, "sp_1": lax.div(m, 2), "sp_2": lax.rem(m, 2)}

    barrier = pltpu.get_barrier_semaphore()

    loads = [
        pltpu.make_async_copy(src, dst, w_sem.at[k])
        for k, (src, dst) in enumerate((
            (ids_hbm, ids_ref), (wts_hbm, wts_ref), (min_hbm, min_ref), (cot_hbm, cot_ref),
            (ix_hbm, ix_ref), (ib_hbm, ib_ref), (ic_hbm, ic_ref), (gz_hbm, gz_ref),
            (raw_hbm, raw_ref), (decay_hbm, decay_ref), (skip_hbm, skip_ref), (gain_hbm, gain_ref),
            (gw_hbm, gw), (uw_hbm, uw), (dw_hbm, dw), (wo_hbm, wo),
        ))
    ]
    for load in loads[:4]:
        load.start()

    def greet(i, carry):
        zz, m = lax.div(i, 8), lax.rem(i, 8)

        @pl.when(i != sp)
        def _():
            pl.semaphore_signal(barrier, inc=1, device_id=peer(zz, m), device_id_type=MESH)

        return carry

    lax.fori_loop(0, PEERS, greet, 0)
    for side in (right, left):
        pl.semaphore_signal(barrier, inc=1, device_id={"tp": side}, device_id_type=MESH)

    for load in loads[4:]:
        load.start()
    for load in loads[:4]:
        load.wait()

    ids = ids_ref[...]
    wts = wts_ref[...]
    place = tok_slots(ids)
    tokens_in = min_ref[...]
    tokens_gr = cot_ref[...]

    def build(i, carry):
        base = (i * 64).astype(F32)
        slot = base + lax.broadcasted_iota(jnp.int32, (64, 128), 0).astype(F32)
        hits = [slot == jnp.broadcast_to(place[k], (64, 128)) for k in (0, 1)]
        pick = (hits[0] | hits[1]).astype(F32)
        weight = jnp.sum(
            jnp.where(hits[0], jnp.broadcast_to(wts[0:1, :], (64, 128)), 0.0)
            + jnp.where(hits[1], jnp.broadcast_to(wts[1:2, :], (64, 128)), 0.0),
            axis=1, keepdims=True,
        )
        pick = pick.astype(BF16)
        part_in = mm(pick, tokens_in).reshape(8, 8, 512)
        part_gr = (mm(pick, tokens_gr) * weight).reshape(8, 8, 512)
        sendbuf[pl.ds(i * 8, 8)] = jnp.concatenate([part_in, part_gr], axis=1).astype(BF16)
        return carry

    lax.fori_loop(0, 8, build, 0)
    ybuf[x, sp] = sendbuf[sp]

    pl.semaphore_wait(barrier, PEERS - 1 + 2)

    def dispatch(i, carry):
        zz = lax.rem(z + NZ - offset_at(lax.div(i, 8)), NZ)
        m = lax.rem(me_yc + lax.rem(i, 8), 8)

        @pl.when(i != 0)
        def _():
            pltpu.make_async_remote_copy(
                src_ref=sendbuf.at[zz * 8 + m], dst_ref=ybuf.at[x, sp],
                send_sem=disp_ss.at[0], recv_sem=disp_rs.at[z],
                device_id=peer(zz, m), device_id_type=MESH,
            ).start()

        return carry

    lax.fori_loop(0, 8, dispatch, 0)

    def waiter(blk, ssem, rsem):
        return pltpu.make_async_remote_copy(
            src_ref=blk, dst_ref=blk, send_sem=ssem, recv_sem=rsem,
            device_id={"tp": right}, device_id_type=MESH,
        )

    def plane_copy(buf, count, zz, ssem, rsem):
        return waiter(buf.at[pl.ds(zz * 8, count)], ssem.at[0], rsem.at[zz])

    def to_side(d, src, dst, ssem, rsem):
        return pltpu.make_async_remote_copy(
            src_ref=src, dst_ref=dst, send_sem=ssem, recv_sem=rsem,
            device_id={"tp": right if d == 0 else left}, device_id_type=MESH,
        )

    def a1(d, zz):
        blk = ybuf.at[x, pl.ds(zz * 8, 8)]
        return to_side(d, blk, blk, a1_s.at[0], a1_r.at[d, zz])

    def a2(d, zz):
        blk = ybuf.at[left if d == 0 else right, pl.ds(zz * 8 + 4 * d, 4)]
        return to_side(d, blk, blk, a2_s.at[0], a2_r.at[zz])

    def r1(d, zz):
        return to_side(d, rs1_s.at[d, zz], rs1_r.at[d, zz], r1_s.at[0], r1_r.at[d, zz])

    def r2(d, zz):
        return to_side(d, rs2_s.at[d, zz], rs2_r.at[d, zz], r2_s.at[0], r2_r.at[zz])


    def group_send(buf, land, m, ssem, rsem):
        return pltpu.make_async_remote_copy(
            src_ref=buf.at[m], dst_ref=land.at[me_yc], send_sem=ssem, recv_sem=rsem,
            device_id=peer(z, m), device_id_type=MESH,
        )

    def plane_send(src, land, zz, ssem, rsem):
        return pltpu.make_async_remote_copy(
            src_ref=src, dst_ref=land.at[z], send_sem=ssem, recv_sem=rsem,
            device_id=peer(zz, me_yc), device_id_type=MESH,
        )

    def seven(buf, ssem, rsem):
        blk = buf.at[pl.ds(0, 7)]
        return pltpu.make_async_remote_copy(
            src_ref=blk, dst_ref=blk, send_sem=ssem, recv_sem=rsem,
            device_id={"tp": right}, device_id_type=MESH,
        )

    def scan_a(state, dec):
        full = jnp.concatenate([state, two_rows(dec)], axis=0).astype(BF16)
        for j in range(8):
            msg_a[j] = full[:, j * 128 : (j + 1) * 128]
        rec_a[me_yc] = msg_a[me_yc]

        def go(t, carry):
            m = lax.rem(me_yc + t, 8)
            group_send(msg_a, rec_a, m, sa_s.at[0], sa_r.at[0]).start()
            return carry

        lax.fori_loop(1, 8, go, 0)

    def scan_b():
        seven(rec_a, sa_s.at[0], sa_r.at[0]).wait_recv()
        state = jnp.zeros((64, 128), F32)
        dec = jnp.ones((1, 128), F32)
        for m in up_order:
            pref[m] = state
            prefd[m] = jnp.broadcast_to(dec, (8, 128))
            tail = rec_a[m, 64:80].astype(F32)
            own = tail[0:1] + tail[1:2]
            state = state * own + rec_a[m, 0:64].astype(F32)
            dec = dec * own
        msg_b[...] = jnp.concatenate([state, two_rows(dec)], axis=0).astype(BF16)
        rec_b[z] = msg_b[...]

        def go(t, carry):
            zz = lax.rem(z + t, NZ)
            plane_send(msg_b, rec_b, zz, sb_s.at[0], sb_r.at[0]).start()
            return carry

        lax.fori_loop(1, NZ, go, 0)

    def scan_c():
        seven(rec_b, sb_s.at[0], sb_r.at[0]).wait_recv()
        state = jnp.zeros((64, 128), F32)
        for zz in up_order:
            tail = rec_b[zz, 64:80].astype(F32)
            nxt = state * (tail[0:1] + tail[1:2]) + rec_b[zz, 0:64].astype(F32)
            state = jnp.where(zz < z, nxt, state)
        for m in range(8):
            msg_c[0, m] = (state * prefd[m][0:1] + pref[m]).astype(BF16)
        rec_c[0, me_yc] = msg_c[0, me_yc]

        def go(t, carry):
            m = lax.rem(me_yc + t, 8)
            group_send(msg_c.at[0], rec_c.at[0], m, sc_s.at[0], sc_r.at[0]).start()
            return carry

        lax.fori_loop(1, 8, go, 0)

    def scan_d(k):
        seven(rec_c.at[k], sc_s.at[k], sc_r.at[k]).wait_recv()
        return jnp.concatenate([rec_c[k, j] for j in range(8)], axis=1)

    up_order = tuple(range(8))
    down_order = tuple(reversed(range(8)))

    def decay_row(tail):
        tail = tail.astype(F32)
        return tail[0:1] + tail[1:2]

    def back_a(state):
        full = state.astype(BF16)
        for j in range(8):
            bmsg_a[j] = full[:, j * 128 : (j + 1) * 128]
        brec_a[me_yc] = bmsg_a[me_yc]

        def go(t, carry):
            m = lax.rem(me_yc + t, 8)
            group_send(bmsg_a, brec_a, m, sa_s.at[1], sa_r.at[1]).start()
            return carry

        lax.fori_loop(1, 8, go, 0)

    def back_send(zz):
        return pltpu.make_async_remote_copy(
            src_ref=bmsg_b, dst_ref=brec_b.at[z], send_sem=bb_s.at[zz], recv_sem=bb_r.at[z],
            device_id=peer(zz, me_yc), device_id_type=MESH,
        )

    def back_recv(zz):
        return pltpu.make_async_remote_copy(
            src_ref=bmsg_b, dst_ref=brec_b.at[zz], send_sem=bb_s.at[zz], recv_sem=bb_r.at[zz],
            device_id={"tp": right}, device_id_type=MESH,
        )

    def back_b():
        seven(brec_a, sa_s.at[1], sa_r.at[1]).wait_recv()
        state = jnp.zeros((64, 128), F32)
        dec = jnp.ones((1, 128), F32)
        for m in down_order:
            pref[m] = state
            prefd[m] = jnp.broadcast_to(dec, (8, 128))
            own = decay_row(rec_a[m, 64:80])
            state = state * own + brec_a[m].astype(F32)
            dec = dec * own
        bmsg_b[...] = state.astype(BF16)
        for zz in down_order:

            @pl.when(zz < z)
            def _():
                back_send(zz).start()

    def back_c():
        carried_back[...] = jnp.zeros((64, 128), F32)
        for zz in down_order[:-1]:

            @pl.when(zz > z)
            def _():
                back_recv(zz).wait_recv()
                carried_back[...] = carried_back[...] * decay_row(rec_b[zz, 64:80]) + brec_b[
                    zz
                ].astype(F32)

        state = carried_back[...]
        for m in range(8):
            msg_c[1, m] = (state * prefd[m][0:1] + pref[m]).astype(BF16)
        rec_c[1, me_yc] = msg_c[1, me_yc]

        def go(t, carry):
            m = lax.rem(me_yc + t, 8)
            group_send(msg_c.at[1], rec_c.at[1], m, sc_s.at[1], sc_r.at[1]).start()
            return carry

        lax.fori_loop(1, 8, go, 0)

    def mix_prepare():
        for load in loads[4:12]:
            load.wait()
        e = head_map()
        raw = upright(raw_ref[...])
        step_size = jnp.maximum(raw, 0.0) + jnp.log1p(jnp.exp(-jnp.abs(raw)))
        dlog = -step_size * decay_ref[...]
        tri = (iota((128, 128), 0) >= iota((128, 128), 1)).astype(F32).astype(BF16)
        running = tri_sum(tri, dlog)
        r_ref[...] = running
        rt_ref[...] = flat(running)
        stepx = spread(step_size, e)
        stepx_ref[...] = stepx
        erx_ref[...] = spread(jnp.exp(running), e)
        tex = spread(jnp.exp(running[127:128] - running), e)
        tex_ref[...] = tex
        xin = ix_ref[...].astype(F32)
        scaled = xin * sigmoid(xin) * stepx
        scaled_ref[...] = scaled
        bin_ = ib_ref[...].astype(F32).T
        cin = ic_ref[...].astype(F32).T
        b_act = (bin_ * sigmoid(bin_)).astype(BF16)
        c_act = (cin * sigmoid(cin)).astype(BF16)
        scores_ref[...] = mm(c_act, b_act, DIMS_NT)
        fresh = mm(b_act, (scaled * tex).astype(BF16), DIMS_TN)
        scan_a(fresh, erx_ref[127:128, :])

    def pair_forward(p, carry):
        lanes = pl.ds(pl.multiple_of(p * 128, 128), 128)
        sc = scaled_ref[:, lanes]
        low = iota((128, 128), 1) < 64
        causal = iota((128, 128), 0) >= iota((128, 128), 1)
        rhs = jnp.concatenate(
            [jnp.where(low, sc, 0.0).astype(BF16), jnp.where(low, 0.0, sc).astype(BF16)], axis=0
        )
        running = r_ref[...]
        scores = scores_ref[...]
        ms = []
        for k in (0, 1):
            h = 2 * p + k
            col = jnp.sum(jnp.where(iota((128, 16), 1) == h, running, 0.0), axis=1, keepdims=True)
            row = rt_ref[pl.ds(h, 1), :]
            w = jnp.exp(jnp.where(causal, col - row, -1e30))
            w_ref[h] = w
            ms.append((scores * w).astype(BF16))
            m_ref[h] = ms[k]
        inside_ref[:, lanes] = mm(jnp.concatenate(ms, axis=1), rhs)
        return carry

    def skip_lanes():
        return spread(jnp.broadcast_to(skip_ref[...], (8, 16)), head_map())[0:1]

    def mix_norm():
        state = scan_d(0)
        carry_ref[...] = state
        cin = ic_ref[...].astype(F32).T
        c_act = (cin * sigmoid(cin)).astype(BF16)
        carried = mm(c_act, state) * erx_ref[...]
        carried_ref[...] = carried
        xin = ix_ref[...].astype(F32)
        zin = gz_ref[...].astype(F32)
        mixed = inside_ref[...] + carried + xin * sigmoid(xin) * skip_lanes()
        gated = mixed * (zin * sigmoid(zin))
        inv = lax.rsqrt(jnp.mean(gated * gated, axis=1, keepdims=True) + EPS)
        gated_ref[...] = gated
        inv_ref[...] = jnp.broadcast_to(inv, (128, 128))
        nr[me_yc] = (gated * inv * gain_ref[...]).astype(BF16)

    def n1(t):
        dev = {"sp_2": 1 - c} if t == 0 else {"sp_1": lax.rem(y + t, NY)}
        blk = nr.at[me_yc]
        return pltpu.make_async_remote_copy(
            src_ref=blk, dst_ref=blk, send_sem=n_s.at[t], recv_sem=n_r.at[t],
            device_id=dev, device_id_type=MESH,
        )

    def n2(t):
        blk = nr.at[lax.rem(y + NY - t, NY) * 2 + c]
        return pltpu.make_async_remote_copy(
            src_ref=blk, dst_ref=blk, send_sem=n_s.at[3 + t], recv_sem=n_r.at[3 + t],
            device_id={"sp_2": 1 - c}, device_id_type=MESH,
        )

    def step(i, carry):
        def take_plane():
            zz = plane_at(z, i)

            @pl.when(i == 0)
            def _():
                plane_copy(ybuf.at[x], 7, z, disp_ss, disp_rs).wait_recv()

            @pl.when(i > 0)
            def _():
                plane_copy(ybuf.at[x], 8, zz, disp_ss, disp_rs).wait_recv()

            a1(0, zz).start()
            a1(1, zz).start()

            @pl.when(i < 2)
            def _():
                lax.fori_loop(16 * i + 8, 16 * i + 24, dispatch, 0)

            @pl.when(i == 2)
            def _():
                lax.fori_loop(40, 48, dispatch, 0)

            @pl.when(i == 3)
            def _():
                lax.fori_loop(48, PEERS, dispatch, 0)

        pl.when((i < 8) & (i != 1))(take_plane)

        @pl.when((i >= 1) & (i < 9))
        def _():
            zz = plane_at(z, i - 1)
            a1(0, zz).wait_recv()
            a2(0, zz).start()
            a1(1, zz).wait_recv()
            a2(1, zz).start()

        pl.when(i == 1)(take_plane)

        @pl.when((i >= 2) & (i < 10))
        def _():
            zz = plane_at(z, i - 2)

            @pl.when(i == 2)
            def _():
                for load in loads[12:15]:
                    load.wait()

            gate = jnp.zeros((128, 256), F32)
            up = jnp.zeros((128, 256), F32)
            hgrad = jnp.zeros((128, 256), F32)
            for q in (x, left, right, far):
                if q is far:
                    waiter(ybuf.at[far, pl.ds(zz * 8, 8)], a2_s.at[0], a2_r.at[zz]).wait_recv()
                rowsq = ybuf[q, pl.ds(zz * 8, 8)].reshape(128, 512)
                gate += mm(rowsq, gw[q])
                up += mm(rowsq, uw[q])
                hgrad += mm(
                    rowsq, dw[:, pl.ds(pl.multiple_of(q * 512, 512), 512)], DIMS_NT
                )
            gate = gate.reshape(8, 16, 256)[:, :8]
            up = up.reshape(8, 16, 256)[:, :8]
            hgrad = hgrad.reshape(8, 16, 256)[:, 8:]
            sig = 1.0 / (1.0 + jnp.exp(-gate))
            act = gate * sig
            zero = jnp.zeros((8, 8, 256), F32)
            hid[pl.ds(zz * 8, 8)] = jnp.concatenate([zero, act * up], axis=1).astype(BF16)
            gg = hgrad * up * sig * (1.0 + gate * (1.0 - sig))
            ug = hgrad * act
            ggi[pl.ds(zz * 8, 8), :, 0:256] = jnp.concatenate([gg, zero], axis=1).astype(BF16)
            ggi[pl.ds(zz * 8, 8), :, 256:512] = jnp.concatenate([ug, zero], axis=1).astype(BF16)
            ggc = gg.reshape(64, 256).astype(BF16)
            ugc = ug.reshape(64, 256).astype(BF16)

            def terms(q):
                return mm(ggc, gw[q], DIMS_NT) + mm(ugc, uw[q], DIMS_NT)

            away = terms(far).astype(BF16)
            rs1_s[0, zz] = away[:32]
            rs1_s[1, zz] = away[32:]
            r1(0, zz).start()
            r1(1, zz).start()
            nbr_acc[0, zz] = terms(right)
            nbr_acc[1, zz] = terms(left)
            own_acc[zz] = terms(x)

        @pl.when((i >= 3) & (i < 11))
        def _():
            zz = plane_at(z, i - 3)
            r1(0, zz).wait_recv()
            rs2_s[0, zz, 0:32] = (nbr_acc[0, zz, 0:32] + rs1_r[0, zz].astype(F32)).astype(BF16)
            rs2_s[0, zz, 32:64] = nbr_acc[0, zz, 32:64].astype(BF16)
            r2(0, zz).start()
            r1(1, zz).wait_recv()
            rs2_s[1, zz, 0:32] = nbr_acc[1, zz, 0:32].astype(BF16)
            rs2_s[1, zz, 32:64] = (nbr_acc[1, zz, 32:64] + rs1_r[1, zz].astype(F32)).astype(BF16)
            r2(1, zz).start()

        @pl.when(i >= 4)
        def _():
            zz = plane_at(z, i - 4)
            waiter(rs2_r.at[:, zz], r2_s.at[0], r2_r.at[zz]).wait_recv()
            total = own_acc[zz] + rs2_r[0, zz].astype(F32) + rs2_r[1, zz].astype(F32)
            total = total.reshape(8, 8, 512)
            retbuf[pl.ds(zz * 8, 8)] = jnp.concatenate(
                [total[:, :, :256], total[:, :, 256:]], axis=1
            ).astype(BF16)

            @pl.when(i == 4)
            def _():
                backbuf[sp] = retbuf[sp]

            def give(k, inner):
                m = lax.rem(me_yc + k, 8)

                @pl.when((k > 0) | (i > 4))
                def _():
                    pltpu.make_async_remote_copy(
                        src_ref=retbuf.at[zz * 8 + m], dst_ref=backbuf.at[sp],
                        send_sem=ret_ss.at[0], recv_sem=ret_rs.at[z],
                        device_id=peer(zz, m), device_id_type=MESH,
                    ).start()

                return inner

            lax.fori_loop(0, 8, give, 0)

        @pl.when(i == 0)
        def _():
            mix_prepare()

        @pl.when(i == 2)
        def _():
            scan_b()

        @pl.when((i >= 3) & (i < 7))
        def _():
            pair_forward(2 * (i - 3), 0)
            pair_forward(2 * (i - 3) + 1, 0)

        @pl.when(i == 4)
        def _():
            scan_c()

        @pl.when(i == 7)
        def _():
            mix_norm()
            for t in range(4):
                n1(t).start()

        return carry

    lax.fori_loop(0, 12, step, 0)

    def weights_in(q):
        g = mm(ybuf[q].reshape(1024, 512), ggi[...].reshape(1024, 512), DIMS_TN)
        gwg_ref[q] = g[:, :256].astype(BF16)
        uwg_ref[q] = g[:, 256:].astype(BF16)

    def weights_down(q):
        d = mm(hid[...].reshape(1024, 256), ybuf[q].reshape(1024, 512), DIMS_TN)
        dout[:, q * 512 : (q + 1) * 512] = d.astype(BF16)

    weights_in(0)
    weights_in(1)
    for t in range(1, 4):
        n1(t).wait_recv()
        n2(t).start()
    weights_in(2)
    weights_in(3)

    def arrive(k, carry):
        zz = plane_at(z, k)

        @pl.when(k == 0)
        def _():
            plane_copy(backbuf, 7, z, ret_ss, ret_rs).wait_recv()

        @pl.when(k > 0)
        def _():
            plane_copy(backbuf, 8, zz, ret_ss, ret_rs).wait_recv()

        return carry

    lax.fori_loop(0, NZ, arrive, 0)
    r_iota = lax.broadcasted_iota(jnp.int32, (128, 1024), 1)
    slot_of = ((r_iota // 16) * 8 + r_iota % 8).astype(F32)
    upper = (r_iota % 16) >= 8
    hit = (slot_of == to_column(place[0])) | (slot_of == to_column(place[1]))
    low = (hit & jnp.logical_not(upper)).astype(F32).astype(BF16)
    high = (hit & upper).astype(F32).astype(BF16)
    back = backbuf[...].reshape(1024, 256)
    moe_grad = jnp.concatenate([mm(low, back), mm(high, back)], axis=1)
    rows[x] = (tokens_gr.astype(F32) + moe_grad).astype(BF16)

    def m1(d, half):
        blk = rows.at[x, pl.ds(64 * ((d + half) % 2), 64)]
        return to_side(d, blk, blk, m_s.at[d, half], m_r.at[d, half])

    def m2(d):
        blk = rows.at[left if d == 0 else right, pl.ds(64 * d, 64)]
        return to_side(d, blk, blk, m_s.at[d, 2], m_r.at[d, 2])

    for half in (0, 1):
        for d in (0, 1):
            m1(d, half).start()

    own_t = rows[x].T.reshape(2, 8, 32, 128)
    for j in range(8):
        turned[j] = own_t[:, j]
    tin[x, me_yc] = turned[me_yc]

    def t1_go(t, carry):
        m = lax.rem(me_yc + t, 8)
        group_send(turned, tin.at[x], m, t1_s.at[0], t1_r.at[0]).start()
        return carry

    lax.fori_loop(1, 8, t1_go, 0)

    def u1(d, half):
        blk = tin.at[x, pl.ds(4 * ((d + half) % 2), 4)]
        return to_side(d, blk, blk, u_s.at[d, half], u_r.at[d, half])

    def u2(d):
        blk = tin.at[left if d == 0 else right, pl.ds(4 * d, 4)]
        return to_side(d, blk, blk, u_s.at[d, 2], u_r.at[d, 2])

    loads[15].wait()
    norm_grad = mm(rows[x], wo[x])
    for d in (0, 1):
        m1(d, 0).wait_recv()
        m2(d).start()
    seven(tin.at[x], t1_s.at[0], t1_r.at[0]).wait_recv()
    for half in (0, 1):
        for d in (0, 1):
            u1(d, half).start()
    for d in (0, 1):
        m1(d, 1).wait_recv()
    norm_grad += mm(rows[left], wo[left])
    norm_grad += mm(rows[right], wo[right])
    m2(0).wait_recv()
    m2(1).wait_recv()
    norm_grad += mm(rows[far], wo[far])
    inv = inv_ref[:, 0:1]
    gated = gated_ref[...]
    scale = norm_grad * gain_ref[...]
    dgated = scale * inv - gated * (inv * inv * inv * jnp.mean(gated * scale, axis=1, keepdims=True))
    zin = gz_ref[...].astype(F32)
    zsig = sigmoid(zin)
    dmix = dgated * (zin * zsig)
    dy_ref[...] = dmix
    cin = ic_ref[...].astype(F32).T
    c_sig = sigmoid(cin)
    c_act = (cin * c_sig).astype(BF16)
    leaving = (dmix * erx_ref[...]).astype(BF16)
    back_a(mm(c_act, leaving, DIMS_TN))
    for d in (0, 1):
        u1(d, 0).wait_recv()
        u2(d).start()
    xin = ix_ref[...].astype(F32)
    xsig = sigmoid(xin)
    mixed = inside_ref[...] + carried_ref[...] + xin * xsig * skip_lanes()
    gzz_ref[...] = (dgated * mixed * (zsig * (1.0 + zin * (1.0 - zsig)))).astype(BF16)
    dsc_ref[...] = jnp.zeros((128, 128), F32)

    def pair_back(p, carry):
        lanes = pl.ds(pl.multiple_of(p * 128, 128), 128)
        dy = dy_ref[:, lanes]
        low = iota((128, 128), 1) < 64
        both = jnp.concatenate(
            [jnp.where(low, dy, 0.0).astype(BF16), jnp.where(low, 0.0, dy).astype(BF16)], axis=0
        )
        ds1_ref[:, lanes] = mm(m_ref[pl.ds(2 * p, 2)].reshape(256, 128), both, DIMS_TN)
        dm = mm(both, scaled_ref[:, lanes].astype(BF16), DIMS_NT)
        dsc_ref[...] += dm[:128] * w_ref[2 * p] + dm[128:] * w_ref[2 * p + 1]
        return carry

    lax.fori_loop(0, 4, pair_back, 0)
    n1(0).wait_recv()
    for t in range(1, 4):
        n2(t).wait_recv()
    for d in (0, 1):
        u1(d, 1).wait_recv()
    u2(0).wait_recv()
    u2(1).wait_recv()
    terms_out = mm(tin[:, 0].reshape(256, 128), nr[0])
    for m in range(1, 8):
        terms_out += mm(tin[:, m].reshape(256, 128), nr[m])
    part[...] = terms_out.reshape(8, 32, 1024).astype(BF16)
    back_b()

    def at_plane(t):
        return lax.rem(z + t + NZ, NZ)

    def t2_far(d):
        return pltpu.make_async_remote_copy(
            src_ref=part.at[at_plane(4), pl.ds(16 * d, 16)], dst_ref=far_in.at[d],
            send_sem=t3_s.at[d], recv_sem=t3_r.at[d],
            device_id=peer(at_plane(1 - 2 * d), me_yc), device_id_type=MESH,
        )

    def t2(t):
        zz = at_plane(t)
        return plane_send(part.at[zz], parts_in, zz, t2_s.at[0], t2_r.at[0])

    def six(buf, ssem, rsem):
        blk = buf.at[pl.ds(0, 6)]
        return pltpu.make_async_remote_copy(
            src_ref=blk, dst_ref=blk, send_sem=ssem, recv_sem=rsem,
            device_id={"tp": right}, device_id_type=MESH,
        )

    t2_far(0).start()
    t2_far(1).start()
    for t in (1, -1, 2, -2):
        t2(t).start()
    lax.fori_loop(4, 8, pair_back, 0)
    back_c()
    t2_far(0).wait_recv()
    over = at_plane(3)
    part[over, 0:16] = (part[over, 0:16].astype(F32) + far_in[0].astype(F32)).astype(BF16)
    t2(3).start()
    t2_far(1).wait_recv()
    under = at_plane(-3)
    part[under, 16:32] = (part[under, 16:32].astype(F32) + far_in[1].astype(F32)).astype(BF16)
    t2(-3).start()
    state = carry_ref[...]
    dsc = dsc_ref[...].astype(BF16)
    bin_ = ib_ref[...].astype(F32).T
    b_sig = sigmoid(bin_)
    b_act = (bin_ * b_sig).astype(BF16)
    dc = mm(dsc, b_act) + mm(leaving, state, DIMS_NT)
    gc_ref[...] = (dc * (c_sig * (1.0 + cin * (1.0 - c_sig)))).T
    e = head_map()
    dmix_b = dmix.astype(BF16).astype(F32)
    scaled = scaled_ref[...]
    scaled_b = scaled.astype(BF16).astype(F32)
    ds1 = ds1_ref[...]
    turn = per_head(dmix_b * inside_ref[...] + dmix * carried_ref[...] - scaled_b * ds1, e)
    for q in range(NX):
        weights_down(q)
    after = scan_d(1)
    tex = tex_ref[...]
    ds2 = mm(b_act, after) * tex
    db = mm(dsc, c_act, DIMS_TN) + mm((scaled * tex).astype(BF16), after, DIMS_NT)
    gb_ref[...] = (db * (b_sig * (1.0 + bin_ * (1.0 - b_sig)))).T
    dscaled = ds1 + ds2
    gx_ref[...] = (
        (dscaled * stepx_ref[...] + dmix * skip_lanes()) * (xsig * (1.0 + xin * (1.0 - xsig)))
    ).astype(BF16)
    fade = per_head(scaled * ds2, e)
    at_end = jnp.sum(after.astype(F32) * state.astype(F32), axis=0, keepdims=True)
    at_end = per_head(jnp.broadcast_to(at_end, (8, 1024)), e)[0:1]
    at_end = jnp.sum(fade, axis=0, keepdims=True) + at_end * jnp.exp(r_ref[127:128, :])
    later = (iota((128, 128), 0) <= iota((128, 128), 1)).astype(F32).astype(BF16)
    dlog_grad = tri_sum(later, turn - fade) + at_end
    raw = upright(raw_ref[...])
    dstep = per_head(dscaled * (xin * xsig), e) - dlog_grad * decay_ref[...]
    graw_ref[...] = flat(dstep * sigmoid(raw))
    waiter(sendbuf.at[pl.ds(0, 63)], disp_ss.at[0], disp_rs.at[0]).wait_send()
    waiter(retbuf.at[pl.ds(0, 63)], ret_ss.at[0], ret_rs.at[0]).wait_send()
    waiter(ybuf.at[pl.ds(0, 2)], a1_s.at[0], a1_r.at[0, 0]).wait_send()
    waiter(ybuf.at[0], a2_s.at[0], a2_r.at[0]).wait_send()
    waiter(rs1_s, r1_s.at[0], r1_r.at[0, 0]).wait_send()
    waiter(rs2_s, r2_s.at[0], r2_r.at[0]).wait_send()
    for d in (0, 1):
        m1(d, 0).wait_send()
        m1(d, 1).wait_send()
        m2(d).wait_send()
        u1(d, 0).wait_send()
        u1(d, 1).wait_send()
        u2(d).wait_send()
    seven(msg_a, sa_s.at[0], sa_r.at[0]).wait_send()
    seven(rec_b, sb_s.at[0], sb_r.at[0]).wait_send()
    seven(msg_c.at[0], sc_s.at[0], sc_r.at[0]).wait_send()
    seven(bmsg_a, sa_s.at[1], sa_r.at[1]).wait_send()
    seven(msg_c.at[1], sc_s.at[1], sc_r.at[1]).wait_send()
    for zz in range(NZ - 1):

        @pl.when(zz < z)
        def _():
            back_send(zz).wait_send()

    for t in range(4):
        n1(t).wait_send()
    for t in range(1, 4):
        n2(t).wait_send()
    seven(turned, t1_s.at[0], t1_r.at[0]).wait_send()
    t2_far(0).wait_send()
    t2_far(1).wait_send()
    six(part, t2_s.at[0], t2_r.at[0]).wait_send()
    six(parts_in, t2_s.at[0], t2_r.at[0]).wait_recv()
    total = part[at_plane(0)].astype(F32)
    for t in (1, -1, 2, -2, 3, -3):
        total += parts_in[at_plane(t)].astype(F32)
    go_ref[...] = total


def fused_call(
    moe_input, cotangent, expert_ids, routing_weights, gate_weight, up_weight, down_weight,
    inner_x, inner_b, inner_c, gate_z, step_raw, decay_rate, skip_weight, norm_gain, w_out,
):
    hbm = pl.BlockSpec(memory_space=pl.ANY)
    dma = pltpu.SemaphoreType.DMA
    V = pltpu.VMEM
    S = pltpu.VMEM
    sems = [dma((16,)), dma((1,)), dma((8,)), dma((1,)), dma((8,))]
    one, each, pairs = dma((1,)), dma((8,)), dma((2, 8))
    sems += [one, pairs, one, each, one, pairs, one, each] + [dma((2, 3))] * 2
    wide = V((128, 1024), F32)
    go, gx, gb, gc, gzz, graw, gwg, uwg, dwg = pl.pallas_call(
        fused_kernel,
        name="fused",
        out_shape=(
            S((32, 1024), F32), S((128, 1024), BF16), S((64, 128), F32), S((64, 128), F32),
            S((128, 1024), BF16), S((16, 128), F32),
            S((NX, 512, 256), BF16), S((NX, 512, 256), BF16), S((256, 2048), BF16),
        ),
        in_specs=[pl.BlockSpec(memory_space=pltpu.HBM)] * 16,
        out_specs=(pl.BlockSpec(memory_space=pltpu.VMEM),) * 9,
        scratch_shapes=[
            V((64, 16, 512), BF16), V((NX, 64, 16, 512), BF16),
            V((NX, 512, 256), BF16), V((NX, 512, 256), BF16), V((256, 2048), BF16),
            V((8, 64, 512), F32), V((2, 8, 64, 512), F32),
            V((2, 8, 32, 512), BF16), V((2, 8, 32, 512), BF16),
            V((2, 8, 64, 512), BF16), V((2, 8, 64, 512), BF16),
            V((64, 16, 512), BF16), V((64, 16, 256), BF16),
            V((64, 16, 256), BF16), V((64, 16, 256), BF16),
            V((NX, 128, 512), BF16),
        ] + sems + [
            V((8, 64, 128), BF16), V((8, 64, 128), BF16), V((64, 128), BF16),
            V((8, 64, 128), BF16), V((64, 128), F32), V((2, 16, 1024), BF16),
            dma((8,)), dma((8,)), dma((2,)), dma((2,)),
            V((2, 128), jnp.int32), V((2, 128), F32), V((128, 512), BF16), V((128, 512), BF16),
            V((128, 1024), BF16), V((64, 128), BF16), V((64, 128), BF16), V((128, 1024), BF16),
            V((16, 128), F32), V((1, 16), F32), V((1, 16), F32), V((1, 1024), F32),
            V((NX, 512, 1024), BF16), wide, wide, wide, wide, V((128, 16), F32),
            V((16, 128), F32), V((128, 128), F32), V((16, 128, 128), F32),
            V((16, 128, 128), BF16), wide, V((64, 1024), BF16), wide,
            V((8, 128, 1024), BF16), wide, V((128, 128), F32), wide, wide, V((128, 128), F32),
            V((8, 80, 128), BF16), V((8, 80, 128), BF16), V((80, 128), BF16),
            V((8, 80, 128), BF16), V((2, 8, 64, 128), BF16), V((2, 8, 64, 128), BF16),
            V((8, 64, 128), F32), V((8, 8, 128), F32),
            V((8, 2, 32, 128), BF16), V((NX, 8, 2, 32, 128), BF16),
            V((8, 32, 1024), BF16), V((8, 32, 1024), BF16),
        ] + [dma((2,))] * 6 + [dma((7,))] * 2 + [dma((1,))] * 4 + [dma((2, 3))] * 2,
        compiler_params=pltpu.CompilerParams(
            collective_id=0, has_side_effects=True, vmem_limit_bytes=62900000
        ),
    )(
        expert_ids.T, routing_weights.T, moe_input, cotangent,
        inner_x, inner_b.T, inner_c.T, gate_z, step_raw.T,
        decay_rate.reshape(1, 16), skip_weight.reshape(1, 16), norm_gain.reshape(1, 1024),
        gate_weight.reshape(NX, 512, 256), up_weight.reshape(NX, 512, 256),
        down_weight.reshape(256, 2048), w_out.reshape(NX, 512, 1024),
    )
    gwg, uwg, dwg, go, gx, gb, gc, gzz, graw = handed_over(
        gwg.reshape(2048, 256), uwg.reshape(2048, 256), dwg, go, gx, gb, gc, gzz, graw
    )
    return gwg[None], uwg[None], dwg[None], go, gx, gb.T, gc.T, gzz, graw.T


def hand_over_kernel(*refs):
    count = (len(refs) - 1) // 2
    srcs, dsts, sem = refs[:count], refs[count : 2 * count], refs[2 * count]
    outs = [pltpu.make_async_copy(srcs[k], dsts[k], sem.at[k]) for k in range(count)]
    for k in range(count):
        outs[k].start()
    for k in range(count):
        outs[k].wait()


def handed_over(*arrays):
    count = len(arrays)
    return pl.pallas_call(
        hand_over_kernel,
        name="handover",
        out_shape=tuple(jax.ShapeDtypeStruct(a.shape, a.dtype) for a in arrays),
        in_specs=[pl.BlockSpec(memory_space=pltpu.VMEM)] * count,
        out_specs=(pl.BlockSpec(memory_space=pl.ANY),) * count,
        scratch_shapes=[pltpu.SemaphoreType.DMA((count,))],
        compiler_params=pltpu.CompilerParams(vmem_limit_bytes=16 * 1024 * 1024),
    )(*arrays)


def solution(mesh):
    finer = Mesh(mesh.devices.reshape(8, 4, 2, mesh.shape["tp"]), ("sp_0", "sp_1", "sp_2", "tp"))
    return jax.shard_map(
        fused_call,
        mesh=finer,
        in_specs=(
            P(SP, "tp"),
            P(SP, "tp"),
            P(SP, None),
            P(SP, None),
            P(SP, None, "tp"),
            P(SP, None, "tp"),
            P(SP, "tp", None),
            P(SP, "tp"),
            P(SP, "tp"),
            P(SP, "tp"),
            P(SP, "tp"),
            P(SP, "tp"),
            P("tp"),
            P("tp"),
            P("tp"),
            P(None, "tp"),
        ),
        out_specs=(
            P(SP, None, "tp"),
            P(SP, None, "tp"),
            P(SP, "tp", None),
            P(SP, "tp"),
            P(SP, "tp"),
            P(SP, "tp"),
            P(SP, "tp"),
            P(SP, "tp"),
            P(SP, "tp"),
        ),
        check_vma=False,
    )
```

```python
import jax
import jax.numpy as jnp
from jax import lax
from jax.experimental import pallas as pl
from jax.experimental.pallas import tpu as pltpu
from jax.sharding import Mesh
from jax.sharding import PartitionSpec as P

SP = ("sp_0", "sp_1", "sp_2")

NZ, NY, NC, NX = 8, 4, 2, 4
PEERS = 64
DIMS_TN = (((0,), (0,)), ((), ()))
DIMS_NT = (((1,), (1,)), ((), ()))
DIMS_NN = (((1,), (0,)), ((), ()))
F32 = jnp.float32
BF16 = jnp.bfloat16
MESH = pl.DeviceIdType.MESH


def mm(a, b, dims=DIMS_NN):
    return lax.dot_general(a, b, dims, preferred_element_type=F32)


def offset_at(i):
    off = jnp.int32(0)
    for k, at in enumerate((0, 1, 7, 2, 6, 4, 3, 5)):
        off = jnp.where(i == k, at, off)
    return off


def plane_at(z, i):
    return lax.rem(z + offset_at(i), NZ)


def tok_slots(ids):
    e_iota = lax.broadcasted_iota(jnp.int32, (PEERS, 128), 0)
    hot = [(jnp.broadcast_to(ids[k : k + 1, :], (PEERS, 128)) == e_iota).astype(F32) for k in (0, 1)]
    earlier = (
        lax.broadcasted_iota(jnp.int32, (128, 128), 0) < lax.broadcasted_iota(jnp.int32, (128, 128), 1)
    ).astype(BF16)
    counts = mm((hot[0] + hot[1]).astype(BF16), earlier)
    return [
        ids[k : k + 1, :].astype(F32) * 8.0 + jnp.sum(hot[k] * counts, axis=0, keepdims=True)
        for k in (0, 1)
    ]


def to_column(row):
    eye = lax.broadcasted_iota(jnp.int32, (128, 128), 0) == lax.broadcasted_iota(
        jnp.int32, (128, 128), 1
    )
    return jnp.sum(jnp.where(eye, jnp.broadcast_to(row, (128, 128)), 0.0), axis=1, keepdims=True)


EPS = 0.01


def split2(v):
    hi = v.astype(BF16)
    return hi, (v - hi.astype(F32)).astype(BF16)


def spread(v, e):
    hi, lo = split2(v)
    return mm(hi, e) + mm(lo, e)


def per_head(v, e):
    hi, lo = split2(v)
    return mm(hi, e, DIMS_NT) + mm(lo, e, DIMS_NT)


def tri_sum(tri, v):
    hi = v.astype(BF16)
    rest = v - hi.astype(F32)
    mid = rest.astype(BF16)
    lo = (rest - mid.astype(F32)).astype(BF16)
    return mm(tri, hi) + mm(tri, mid) + mm(tri, lo)


def sigmoid(v):
    return 1.0 / (1.0 + jnp.exp(-v))


def iota(shape, dim):
    return lax.broadcasted_iota(jnp.int32, shape, dim)


def head_map():
    return (lax.div(iota((16, 1024), 1), 64) == iota((16, 1024), 0)).astype(F32).astype(BF16)


def upright(narrow):
    return jnp.concatenate([narrow, jnp.zeros((112, 128), F32)], axis=0).T[:, 0:16]


def flat(narrow):
    return jnp.concatenate([narrow, jnp.zeros((128, 112), F32)], axis=1).T[0:16]


def two_rows(dec):
    hi = dec.astype(BF16).astype(F32)
    row = iota((16, dec.shape[1]), 0)
    return jnp.where(row == 0, hi, jnp.where(row == 1, dec - hi, 0.0))


def fused_kernel(
    ids_hbm, wts_hbm, min_hbm, cot_hbm, ix_hbm, ib_hbm, ic_hbm, gz_hbm, raw_hbm, decay_hbm,
    skip_hbm, gain_hbm, gw_hbm, uw_hbm, dw_hbm, wo_hbm,
    go_ref, gx_ref, gb_ref, gc_ref, gzz_ref, graw_ref, gwg_ref, uwg_ref, dout,
    sendbuf, ybuf, gw, uw, dw, own_acc, nbr_acc, rs1_s, rs1_r, rs2_s, rs2_r,
    ggi, hid, retbuf, backbuf, rows,
    w_sem, disp_ss, disp_rs, ret_ss, ret_rs,
    a1_s, a1_r, a2_s, a2_r, r1_s, r1_r, r2_s, r2_r, m_s, m_r,
    bmsg_a, brec_a, bmsg_b, brec_b,
    carried_back, far_in, bb_s, bb_r, t3_s, t3_r,
    ids_ref, wts_ref, min_ref, cot_ref, ix_ref, ib_ref, ic_ref, gz_ref, raw_ref, decay_ref,
    skip_ref, gain_ref, wo, scaled_ref, stepx_ref, erx_ref, tex_ref, r_ref, rt_ref, scores_ref, w_ref, m_ref,
    inside_ref, carry_ref, carried_ref, nr, gated_ref, inv_ref, dy_ref, ds1_ref, dsc_ref,
    msg_a, rec_a, msg_b, rec_b, msg_c, rec_c, pref, prefd, turned, tin, part, parts_in,
    sa_s, sa_r, sb_s, sb_r, sc_s, sc_r, n_s, n_r, t1_s, t1_r, t2_s, t2_r, u_s, u_r,
):
    z, y, c, x = (lax.axis_index(a) for a in ("sp_0", "sp_1", "sp_2", "tp"))
    sp = z * 8 + y * 2 + c
    me_yc = y * 2 + c
    right, left = lax.rem(x + 1, NX), lax.rem(x + 3, NX)
    far = lax.rem(x + 2, NX)

    def peer(zz, m):
        return {"sp_0": zz, "sp_1": lax.div(m, 2), "sp_2": lax.rem(m, 2)}

    barrier = pltpu.get_barrier_semaphore()

    loads = [
        pltpu.make_async_copy(src, dst, w_sem.at[k])
        for k, (src, dst) in enumerate((
            (ids_hbm, ids_ref), (wts_hbm, wts_ref), (min_hbm, min_ref), (cot_hbm, cot_ref),
            (ix_hbm, ix_ref), (ib_hbm, ib_ref), (ic_hbm, ic_ref), (gz_hbm, gz_ref),
            (raw_hbm, raw_ref), (decay_hbm, decay_ref), (skip_hbm, skip_ref), (gain_hbm, gain_ref),
            (gw_hbm, gw), (uw_hbm, uw), (dw_hbm, dw), (wo_hbm, wo),
        ))
    ]
    for load in loads[:4]:
        load.start()

    def greet(i, carry):
        zz, m = lax.div(i, 8), lax.rem(i, 8)

        @pl.when(i != sp)
        def _():
            pl.semaphore_signal(barrier, inc=1, device_id=peer(zz, m), device_id_type=MESH)

        return carry

    lax.fori_loop(0, PEERS, greet, 0)
    for side in (right, left):
        pl.semaphore_signal(barrier, inc=1, device_id={"tp": side}, device_id_type=MESH)

    for load in loads[4:]:
        load.start()
    for load in loads[:4]:
        load.wait()

    ids = ids_ref[...]
    wts = wts_ref[...]
    place = tok_slots(ids)
    tokens_in = min_ref[...]
    tokens_gr = cot_ref[...]

    def build(i, carry):
        base = (i * 64).astype(F32)
        slot = base + lax.broadcasted_iota(jnp.int32, (64, 128), 0).astype(F32)
        hits = [slot == jnp.broadcast_to(place[k], (64, 128)) for k in (0, 1)]
        pick = (hits[0] | hits[1]).astype(F32)
        weight = jnp.sum(
            jnp.where(hits[0], jnp.broadcast_to(wts[0:1, :], (64, 128)), 0.0)
            + jnp.where(hits[1], jnp.broadcast_to(wts[1:2, :], (64, 128)), 0.0),
            axis=1, keepdims=True,
        )
        pick = pick.astype(BF16)
        part_in = mm(pick, tokens_in).reshape(8, 8, 512)
        part_gr = (mm(pick, tokens_gr) * weight).reshape(8, 8, 512)
        sendbuf[pl.ds(i * 8, 8)] = jnp.concatenate([part_in, part_gr], axis=1).astype(BF16)
        return carry

    lax.fori_loop(0, 8, build, 0)
    ybuf[x, sp] = sendbuf[sp]

    pl.semaphore_wait(barrier, PEERS - 1 + 2)

    def dispatch(i, carry):
        zz = lax.rem(z + NZ - offset_at(lax.div(i, 8)), NZ)
        m = lax.rem(me_yc + lax.rem(i, 8), 8)

        @pl.when(i != 0)
        def _():
            pltpu.make_async_remote_copy(
                src_ref=sendbuf.at[zz * 8 + m], dst_ref=ybuf.at[x, sp],
                send_sem=disp_ss.at[0], recv_sem=disp_rs.at[z],
                device_id=peer(zz, m), device_id_type=MESH,
            ).start()

        return carry

    lax.fori_loop(0, 8, dispatch, 0)

    def waiter(blk, ssem, rsem):
        return pltpu.make_async_remote_copy(
            src_ref=blk, dst_ref=blk, send_sem=ssem, recv_sem=rsem,
            device_id={"tp": right}, device_id_type=MESH,
        )

    def plane_copy(buf, count, zz, ssem, rsem):
        return waiter(buf.at[pl.ds(zz * 8, count)], ssem.at[0], rsem.at[zz])

    def to_side(d, src, dst, ssem, rsem):
        return pltpu.make_async_remote_copy(
            src_ref=src, dst_ref=dst, send_sem=ssem, recv_sem=rsem,
            device_id={"tp": right if d == 0 else left}, device_id_type=MESH,
        )

    def a1(d, zz):
        blk = ybuf.at[x, pl.ds(zz * 8, 8)]
        return to_side(d, blk, blk, a1_s.at[0], a1_r.at[d, zz])

    def a2(d, zz):
        blk = ybuf.at[left if d == 0 else right, pl.ds(zz * 8 + 4 * d, 4)]
        return to_side(d, blk, blk, a2_s.at[0], a2_r.at[zz])

    def r1(d, zz):
        return to_side(d, rs1_s.at[d, zz], rs1_r.at[d, zz], r1_s.at[0], r1_r.at[d, zz])

    def r2(d, zz):
        return to_side(d, rs2_s.at[d, zz], rs2_r.at[d, zz], r2_s.at[0], r2_r.at[zz])


    def group_send(buf, land, m, ssem, rsem):
        return pltpu.make_async_remote_copy(
            src_ref=buf.at[m], dst_ref=land.at[me_yc], send_sem=ssem, recv_sem=rsem,
            device_id=peer(z, m), device_id_type=MESH,
        )

    def plane_send(src, land, zz, ssem, rsem):
        return pltpu.make_async_remote_copy(
            src_ref=src, dst_ref=land.at[z], send_sem=ssem, recv_sem=rsem,
            device_id=peer(zz, me_yc), device_id_type=MESH,
        )

    def seven(buf, ssem, rsem):
        blk = buf.at[pl.ds(0, 7)]
        return pltpu.make_async_remote_copy(
            src_ref=blk, dst_ref=blk, send_sem=ssem, recv_sem=rsem,
            device_id={"tp": right}, device_id_type=MESH,
        )

    def scan_a(state, dec):
        full = jnp.concatenate([state, two_rows(dec)], axis=0).astype(BF16)
        for j in range(8):
            msg_a[j] = full[:, j * 128 : (j + 1) * 128]
        rec_a[me_yc] = msg_a[me_yc]

        def go(t, carry):
            m = lax.rem(me_yc + lax.rem(t + 1, 7) + 1, 8)
            group_send(msg_a, rec_a, m, sa_s.at[0], sa_r.at[0]).start()
            return carry

        lax.fori_loop(1, 8, go, 0)

    def scan_b():
        seven(rec_a, sa_s.at[0], sa_r.at[0]).wait_recv()
        state = jnp.zeros((64, 128), F32)
        dec = jnp.ones((1, 128), F32)
        for m in up_order:
            pref[m] = state
            prefd[m] = jnp.broadcast_to(dec, (8, 128))
            tail = rec_a[m, 64:80].astype(F32)
            own = tail[0:1] + tail[1:2]
            state = state * own + rec_a[m, 0:64].astype(F32)
            dec = dec * own
        msg_b[...] = jnp.concatenate([state, two_rows(dec)], axis=0).astype(BF16)
        rec_b[z] = msg_b[...]

        def go(t, carry):
            zz = lax.rem(z + t, NZ)
            plane_send(msg_b, rec_b, zz, sb_s.at[0], sb_r.at[0]).start()
            return carry

        lax.fori_loop(1, NZ, go, 0)

    def scan_c():
        seven(rec_b, sb_s.at[0], sb_r.at[0]).wait_recv()
        state = jnp.zeros((64, 128), F32)
        for zz in up_order:
            tail = rec_b[zz, 64:80].astype(F32)
            nxt = state * (tail[0:1] + tail[1:2]) + rec_b[zz, 0:64].astype(F32)
            state = jnp.where(zz < z, nxt, state)
        for m in range(8):
            msg_c[0, m] = (state * prefd[m][0:1] + pref[m]).astype(BF16)
        rec_c[0, me_yc] = msg_c[0, me_yc]

        def go(t, carry):
            m = lax.rem(me_yc + lax.rem(t + 1, 7) + 1, 8)
            group_send(msg_c.at[0], rec_c.at[0], m, sc_s.at[0], sc_r.at[0]).start()
            return carry

        lax.fori_loop(1, 8, go, 0)

    def scan_d(k):
        seven(rec_c.at[k], sc_s.at[k], sc_r.at[k]).wait_recv()
        return jnp.concatenate([rec_c[k, j] for j in range(8)], axis=1)

    up_order = tuple(range(8))
    down_order = tuple(reversed(range(8)))

    def decay_row(tail):
        tail = tail.astype(F32)
        return tail[0:1] + tail[1:2]

    def back_a(state):
        full = state.astype(BF16)
        for j in range(8):
            bmsg_a[j] = full[:, j * 128 : (j + 1) * 128]
        brec_a[me_yc] = bmsg_a[me_yc]

        def go(t, carry):
            m = lax.rem(me_yc + lax.rem(t + 1, 7) + 1, 8)
            group_send(bmsg_a, brec_a, m, sa_s.at[1], sa_r.at[1]).start()
            return carry

        lax.fori_loop(1, 8, go, 0)

    def back_send(zz):
        return pltpu.make_async_remote_copy(
            src_ref=bmsg_b, dst_ref=brec_b.at[z], send_sem=bb_s.at[zz], recv_sem=bb_r.at[z],
            device_id=peer(zz, me_yc), device_id_type=MESH,
        )

    def back_recv(zz):
        return pltpu.make_async_remote_copy(
            src_ref=bmsg_b, dst_ref=brec_b.at[zz], send_sem=bb_s.at[zz], recv_sem=bb_r.at[zz],
            device_id={"tp": right}, device_id_type=MESH,
        )

    def back_b():
        seven(brec_a, sa_s.at[1], sa_r.at[1]).wait_recv()
        state = jnp.zeros((64, 128), F32)
        dec = jnp.ones((1, 128), F32)
        for m in down_order:
            pref[m] = state
            prefd[m] = jnp.broadcast_to(dec, (8, 128))
            own = decay_row(rec_a[m, 64:80])
            state = state * own + brec_a[m].astype(F32)
            dec = dec * own
        bmsg_b[...] = state.astype(BF16)
        for zz in down_order:

            @pl.when(zz < z)
            def _():
                back_send(zz).start()

    def back_c():
        carried_back[...] = jnp.zeros((64, 128), F32)
        for zz in down_order[:-1]:

            @pl.when(zz > z)
            def _():
                back_recv(zz).wait_recv()
                carried_back[...] = carried_back[...] * decay_row(rec_b[zz, 64:80]) + brec_b[
                    zz
                ].astype(F32)

        state = carried_back[...]
        for m in range(8):
            msg_c[1, m] = (state * prefd[m][0:1] + pref[m]).astype(BF16)
        rec_c[1, me_yc] = msg_c[1, me_yc]

        def go(t, carry):
            m = lax.rem(me_yc + lax.rem(t + 1, 7) + 1, 8)
            group_send(msg_c.at[1], rec_c.at[1], m, sc_s.at[1], sc_r.at[1]).start()
            return carry

        lax.fori_loop(1, 8, go, 0)

    def mix_prepare():
        for load in loads[4:12]:
            load.wait()
        e = head_map()
        raw = upright(raw_ref[...])
        step_size = jnp.maximum(raw, 0.0) + jnp.log1p(jnp.exp(-jnp.abs(raw)))
        dlog = -step_size * decay_ref[...]
        tri = (iota((128, 128), 0) >= iota((128, 128), 1)).astype(F32).astype(BF16)
        running = tri_sum(tri, dlog)
        r_ref[...] = running
        rt_ref[...] = flat(running)
        stepx = spread(step_size, e)
        stepx_ref[...] = stepx
        erx_ref[...] = spread(jnp.exp(running), e)
        tex = spread(jnp.exp(running[127:128] - running), e)
        tex_ref[...] = tex
        xin = ix_ref[...].astype(F32)
        scaled = xin * sigmoid(xin) * stepx
        scaled_ref[...] = scaled
        bin_ = ib_ref[...].astype(F32).T
        cin = ic_ref[...].astype(F32).T
        b_act = (bin_ * sigmoid(bin_)).astype(BF16)
        c_act = (cin * sigmoid(cin)).astype(BF16)
        scores_ref[...] = mm(c_act, b_act, DIMS_NT)
        fresh = mm(b_act, (scaled * tex).astype(BF16), DIMS_TN)
        scan_a(fresh, erx_ref[127:128, :])

    def pair_forward(p, carry):
        lanes = pl.ds(pl.multiple_of(p * 128, 128), 128)
        sc = scaled_ref[:, lanes]
        low = iota((128, 128), 1) < 64
        causal = iota((128, 128), 0) >= iota((128, 128), 1)
        rhs = jnp.concatenate(
            [jnp.where(low, sc, 0.0).astype(BF16), jnp.where(low, 0.0, sc).astype(BF16)], axis=0
        )
        running = r_ref[...]
        scores = scores_ref[...]
        ms = []
        for k in (0, 1):
            h = 2 * p + k
            col = jnp.sum(jnp.where(iota((128, 16), 1) == h, running, 0.0), axis=1, keepdims=True)
            row = rt_ref[pl.ds(h, 1), :]
            w = jnp.exp(jnp.where(causal, col - row, -1e30))
            w_ref[h] = w
            ms.append((scores * w).astype(BF16))
            m_ref[h] = ms[k]
        inside_ref[:, lanes] = mm(jnp.concatenate(ms, axis=1), rhs)
        return carry

    def skip_lanes():
        return spread(jnp.broadcast_to(skip_ref[...], (8, 16)), head_map())[0:1]

    def mix_norm():
        state = scan_d(0)
        carry_ref[...] = state
        cin = ic_ref[...].astype(F32).T
        c_act = (cin * sigmoid(cin)).astype(BF16)
        carried = mm(c_act, state) * erx_ref[...]
        carried_ref[...] = carried
        xin = ix_ref[...].astype(F32)
        zin = gz_ref[...].astype(F32)
        mixed = inside_ref[...] + carried + xin * sigmoid(xin) * skip_lanes()
        gated = mixed * (zin * sigmoid(zin))
        inv = lax.rsqrt(jnp.mean(gated * gated, axis=1, keepdims=True) + EPS)
        gated_ref[...] = gated
        inv_ref[...] = jnp.broadcast_to(inv, (128, 128))
        nr[me_yc] = (gated * inv * gain_ref[...]).astype(BF16)

    def n1(t):
        dev = {"sp_2": 1 - c} if t == 0 else {"sp_1": lax.rem(y + t, NY)}
        blk = nr.at[me_yc]
        return pltpu.make_async_remote_copy(
            src_ref=blk, dst_ref=blk, send_sem=n_s.at[t], recv_sem=n_r.at[t],
            device_id=dev, device_id_type=MESH,
        )

    def n2(t):
        blk = nr.at[lax.rem(y + NY - t, NY) * 2 + c]
        return pltpu.make_async_remote_copy(
            src_ref=blk, dst_ref=blk, send_sem=n_s.at[3 + t], recv_sem=n_r.at[3 + t],
            device_id={"sp_2": 1 - c}, device_id_type=MESH,
        )

    def step(i, carry):
        def take_plane():
            zz = plane_at(z, i)

            @pl.when(i == 0)
            def _():
                plane_copy(ybuf.at[x], 7, z, disp_ss, disp_rs).wait_recv()

            @pl.when(i > 0)
            def _():
                plane_copy(ybuf.at[x], 8, zz, disp_ss, disp_rs).wait_recv()

            a1(0, zz).start()
            a1(1, zz).start()

            @pl.when(i < 2)
            def _():
                lax.fori_loop(16 * i + 8, 16 * i + 24, dispatch, 0)

            @pl.when(i == 2)
            def _():
                lax.fori_loop(40, 48, dispatch, 0)

            @pl.when(i == 3)
            def _():
                lax.fori_loop(48, PEERS, dispatch, 0)

        pl.when((i < 8) & (i != 1))(take_plane)

        @pl.when((i >= 1) & (i < 9))
        def _():
            zz = plane_at(z, i - 1)
            a1(0, zz).wait_recv()
            a2(0, zz).start()
            a1(1, zz).wait_recv()
            a2(1, zz).start()

        pl.when(i == 1)(take_plane)

        @pl.when((i >= 2) & (i < 10))
        def _():
            zz = plane_at(z, i - 2)

            @pl.when(i == 2)
            def _():
                for load in loads[12:15]:
                    load.wait()

            gate = jnp.zeros((128, 256), F32)
            up = jnp.zeros((128, 256), F32)
            hgrad = jnp.zeros((128, 256), F32)
            for q in (x, left, right, far):
                if q is far:
                    waiter(ybuf.at[far, pl.ds(zz * 8, 8)], a2_s.at[0], a2_r.at[zz]).wait_recv()
                rowsq = ybuf[q, pl.ds(zz * 8, 8)].reshape(128, 512)
                gate += mm(rowsq, gw[q])
                up += mm(rowsq, uw[q])
                hgrad += mm(
                    rowsq, dw[:, pl.ds(pl.multiple_of(q * 512, 512), 512)], DIMS_NT
                )
            gate = gate.reshape(8, 16, 256)[:, :8]
            up = up.reshape(8, 16, 256)[:, :8]
            hgrad = hgrad.reshape(8, 16, 256)[:, 8:]
            sig = 1.0 / (1.0 + jnp.exp(-gate))
            act = gate * sig
            zero = jnp.zeros((8, 8, 256), F32)
            hid[pl.ds(zz * 8, 8)] = jnp.concatenate([zero, act * up], axis=1).astype(BF16)
            gg = hgrad * up * sig * (1.0 + gate * (1.0 - sig))
            ug = hgrad * act
            ggi[pl.ds(zz * 8, 8), :, 0:256] = jnp.concatenate([gg, zero], axis=1).astype(BF16)
            ggi[pl.ds(zz * 8, 8), :, 256:512] = jnp.concatenate([ug, zero], axis=1).astype(BF16)
            ggc = gg.reshape(64, 256).astype(BF16)
            ugc = ug.reshape(64, 256).astype(BF16)

            def terms(q):
                return mm(ggc, gw[q], DIMS_NT) + mm(ugc, uw[q], DIMS_NT)

            away = terms(far).astype(BF16)
            rs1_s[0, zz] = away[:32]
            rs1_s[1, zz] = away[32:]
            r1(0, zz).start()
            r1(1, zz).start()
            nbr_acc[0, zz] = terms(right)
            nbr_acc[1, zz] = terms(left)
            own_acc[zz] = terms(x)

        @pl.when((i >= 3) & (i < 11))
        def _():
            zz = plane_at(z, i - 3)
            r1(0, zz).wait_recv()
            rs2_s[0, zz, 0:32] = (nbr_acc[0, zz, 0:32] + rs1_r[0, zz].astype(F32)).astype(BF16)
            rs2_s[0, zz, 32:64] = nbr_acc[0, zz, 32:64].astype(BF16)
            r2(0, zz).start()
            r1(1, zz).wait_recv()
            rs2_s[1, zz, 0:32] = nbr_acc[1, zz, 0:32].astype(BF16)
            rs2_s[1, zz, 32:64] = (nbr_acc[1, zz, 32:64] + rs1_r[1, zz].astype(F32)).astype(BF16)
            r2(1, zz).start()

        @pl.when(i >= 4)
        def _():
            zz = plane_at(z, i - 4)
            waiter(rs2_r.at[:, zz], r2_s.at[0], r2_r.at[zz]).wait_recv()
            total = own_acc[zz] + rs2_r[0, zz].astype(F32) + rs2_r[1, zz].astype(F32)
            total = total.reshape(8, 8, 512)
            retbuf[pl.ds(zz * 8, 8)] = jnp.concatenate(
                [total[:, :, :256], total[:, :, 256:]], axis=1
            ).astype(BF16)

            @pl.when(i == 4)
            def _():
                backbuf[sp] = retbuf[sp]

            def give(k, inner):
                m = lax.rem(me_yc + k, 8)

                @pl.when((k > 0) | (i > 4))
                def _():
                    pltpu.make_async_remote_copy(
                        src_ref=retbuf.at[zz * 8 + m], dst_ref=backbuf.at[sp],
                        send_sem=ret_ss.at[0], recv_sem=ret_rs.at[z],
                        device_id=peer(zz, m), device_id_type=MESH,
                    ).start()

                return inner

            lax.fori_loop(0, 8, give, 0)

        @pl.when(i == 0)
        def _():
            mix_prepare()

        @pl.when(i == 2)
        def _():
            scan_b()

        @pl.when((i >= 3) & (i < 7))
        def _():
            pair_forward(2 * (i - 3), 0)
            pair_forward(2 * (i - 3) + 1, 0)

        @pl.when(i == 4)
        def _():
            scan_c()

        @pl.when(i == 7)
        def _():
            mix_norm()
            for t in range(4):
                n1(t).start()

        return carry

    lax.fori_loop(0, 12, step, 0)

    def weights_in(q):
        g = mm(ybuf[q].reshape(1024, 512), ggi[...].reshape(1024, 512), DIMS_TN)
        gwg_ref[q] = g[:, :256].astype(BF16)
        uwg_ref[q] = g[:, 256:].astype(BF16)

    def weights_down(q):
        d = mm(hid[...].reshape(1024, 256), ybuf[q].reshape(1024, 512), DIMS_TN)
        dout[:, q * 512 : (q + 1) * 512] = d.astype(BF16)

    weights_in(0)
    weights_in(1)
    for t in range(1, 4):
        n1(t).wait_recv()
        n2(t).start()
    weights_in(2)
    weights_in(3)

    def arrive(k, carry):
        zz = plane_at(z, k)

        @pl.when(k == 0)
        def _():
            plane_copy(backbuf, 7, z, ret_ss, ret_rs).wait_recv()

        @pl.when(k > 0)
        def _():
            plane_copy(backbuf, 8, zz, ret_ss, ret_rs).wait_recv()

        return carry

    lax.fori_loop(0, NZ, arrive, 0)
    r_iota = lax.broadcasted_iota(jnp.int32, (128, 1024), 1)
    slot_of = ((r_iota // 16) * 8 + r_iota % 8).astype(F32)
    upper = (r_iota % 16) >= 8
    hit = (slot_of == to_column(place[0])) | (slot_of == to_column(place[1]))
    low = (hit & jnp.logical_not(upper)).astype(F32).astype(BF16)
    high = (hit & upper).astype(F32).astype(BF16)
    back = backbuf[...].reshape(1024, 256)
    moe_grad = jnp.concatenate([mm(low, back), mm(high, back)], axis=1)
    rows[x] = (tokens_gr.astype(F32) + moe_grad).astype(BF16)

    def m1(d, half):
        blk = rows.at[x, pl.ds(64 * ((d + half) % 2), 64)]
        return to_side(d, blk, blk, m_s.at[d, half], m_r.at[d, half])

    def m2(d):
        blk = rows.at[left if d == 0 else right, pl.ds(64 * d, 64)]
        return to_side(d, blk, blk, m_s.at[d, 2], m_r.at[d, 2])

    for half in (0, 1):
        for d in (0, 1):
            m1(d, half).start()

    own_t = rows[x].T.reshape(2, 8, 32, 128)
    for j in range(8):
        turned[j] = own_t[:, j]
    tin[x, me_yc] = turned[me_yc]

    def t1_go(t, carry):
        m = lax.rem(me_yc + lax.rem(t + 1, 7) + 1, 8)
        group_send(turned, tin.at[x], m, t1_s.at[0], t1_r.at[0]).start()
        return carry

    lax.fori_loop(1, 8, t1_go, 0)

    def u1(d, half):
        blk = tin.at[x, pl.ds(4 * ((d + half) % 2), 4)]
        return to_side(d, blk, blk, u_s.at[d, half], u_r.at[d, half])

    def u2(d):
        blk = tin.at[left if d == 0 else right, pl.ds(4 * d, 4)]
        return to_side(d, blk, blk, u_s.at[d, 2], u_r.at[d, 2])

    loads[15].wait()
    norm_grad = mm(rows[x], wo[x])
    for d in (0, 1):
        m1(d, 0).wait_recv()
        m2(d).start()
    seven(tin.at[x], t1_s.at[0], t1_r.at[0]).wait_recv()
    for half in (0, 1):
        for d in (0, 1):
            u1(d, half).start()
    for d in (0, 1):
        m1(d, 1).wait_recv()
    norm_grad += mm(rows[left], wo[left])
    norm_grad += mm(rows[right], wo[right])
    m2(0).wait_recv()
    m2(1).wait_recv()
    norm_grad += mm(rows[far], wo[far])
    inv = inv_ref[:, 0:1]
    gated = gated_ref[...]
    scale = norm_grad * gain_ref[...]
    dgated = scale * inv - gated * (inv * inv * inv * jnp.mean(gated * scale, axis=1, keepdims=True))
    zin = gz_ref[...].astype(F32)
    zsig = sigmoid(zin)
    dmix = dgated * (zin * zsig)
    dy_ref[...] = dmix
    cin = ic_ref[...].astype(F32).T
    c_sig = sigmoid(cin)
    c_act = (cin * c_sig).astype(BF16)
    leaving = (dmix * erx_ref[...]).astype(BF16)
    back_a(mm(c_act, leaving, DIMS_TN))
    for d in (0, 1):
        u1(d, 0).wait_recv()
        u2(d).start()
    xin = ix_ref[...].astype(F32)
    xsig = sigmoid(xin)
    mixed = inside_ref[...] + carried_ref[...] + xin * xsig * skip_lanes()
    gzz_ref[...] = (dgated * mixed * (zsig * (1.0 + zin * (1.0 - zsig)))).astype(BF16)
    dsc_ref[...] = jnp.zeros((128, 128), F32)

    def pair_back(p, carry):
        lanes = pl.ds(pl.multiple_of(p * 128, 128), 128)
        dy = dy_ref[:, lanes]
        low = iota((128, 128), 1) < 64
        both = jnp.concatenate(
            [jnp.where(low, dy, 0.0).astype(BF16), jnp.where(low, 0.0, dy).astype(BF16)], axis=0
        )
        ds1_ref[:, lanes] = mm(m_ref[pl.ds(2 * p, 2)].reshape(256, 128), both, DIMS_TN)
        dm = mm(both, scaled_ref[:, lanes].astype(BF16), DIMS_NT)
        dsc_ref[...] += dm[:128] * w_ref[2 * p] + dm[128:] * w_ref[2 * p + 1]
        return carry

    lax.fori_loop(0, 4, pair_back, 0)
    n1(0).wait_recv()
    for t in range(1, 4):
        n2(t).wait_recv()
    for d in (0, 1):
        u1(d, 1).wait_recv()
    u2(0).wait_recv()
    u2(1).wait_recv()
    terms_out = mm(tin[:, 0].reshape(256, 128), nr[0])
    for m in range(1, 8):
        terms_out += mm(tin[:, m].reshape(256, 128), nr[m])
    part[...] = terms_out.reshape(8, 32, 1024).astype(BF16)
    back_b()

    def at_plane(t):
        return lax.rem(z + t + NZ, NZ)

    def t2_far(d):
        return pltpu.make_async_remote_copy(
            src_ref=part.at[at_plane(4), pl.ds(16 * d, 16)], dst_ref=far_in.at[d],
            send_sem=t3_s.at[d], recv_sem=t3_r.at[d],
            device_id=peer(at_plane(1 - 2 * d), me_yc), device_id_type=MESH,
        )

    def t2(t):
        zz = at_plane(t)
        return plane_send(part.at[zz], parts_in, zz, t2_s.at[0], t2_r.at[0])

    def six(buf, ssem, rsem):
        blk = buf.at[pl.ds(0, 6)]
        return pltpu.make_async_remote_copy(
            src_ref=blk, dst_ref=blk, send_sem=ssem, recv_sem=rsem,
            device_id={"tp": right}, device_id_type=MESH,
        )

    t2_far(0).start()
    t2_far(1).start()
    for t in (1, -1, 2, -2):
        t2(t).start()
    lax.fori_loop(4, 8, pair_back, 0)
    back_c()
    t2_far(0).wait_recv()
    over = at_plane(3)
    part[over, 0:16] = (part[over, 0:16].astype(F32) + far_in[0].astype(F32)).astype(BF16)
    t2(3).start()
    t2_far(1).wait_recv()
    under = at_plane(-3)
    part[under, 16:32] = (part[under, 16:32].astype(F32) + far_in[1].astype(F32)).astype(BF16)
    t2(-3).start()
    state = carry_ref[...]
    dsc = dsc_ref[...].astype(BF16)
    bin_ = ib_ref[...].astype(F32).T
    b_sig = sigmoid(bin_)
    b_act = (bin_ * b_sig).astype(BF16)
    dc = mm(dsc, b_act) + mm(leaving, state, DIMS_NT)
    gc_ref[...] = (dc * (c_sig * (1.0 + cin * (1.0 - c_sig)))).T
    e = head_map()
    dmix_b = dmix.astype(BF16).astype(F32)
    scaled = scaled_ref[...]
    scaled_b = scaled.astype(BF16).astype(F32)
    ds1 = ds1_ref[...]
    turn = per_head(dmix_b * inside_ref[...] + dmix * carried_ref[...] - scaled_b * ds1, e)
    for q in range(NX):
        weights_down(q)
    after = scan_d(1)
    tex = tex_ref[...]
    ds2 = mm(b_act, after) * tex
    db = mm(dsc, c_act, DIMS_TN) + mm((scaled * tex).astype(BF16), after, DIMS_NT)
    gb_ref[...] = (db * (b_sig * (1.0 + bin_ * (1.0 - b_sig)))).T
    dscaled = ds1 + ds2
    gx_ref[...] = (
        (dscaled * stepx_ref[...] + dmix * skip_lanes()) * (xsig * (1.0 + xin * (1.0 - xsig)))
    ).astype(BF16)
    fade = per_head(scaled * ds2, e)
    at_end = jnp.sum(after.astype(F32) * state.astype(F32), axis=0, keepdims=True)
    at_end = per_head(jnp.broadcast_to(at_end, (8, 1024)), e)[0:1]
    at_end = jnp.sum(fade, axis=0, keepdims=True) + at_end * jnp.exp(r_ref[127:128, :])
    later = (iota((128, 128), 0) <= iota((128, 128), 1)).astype(F32).astype(BF16)
    dlog_grad = tri_sum(later, turn - fade) + at_end
    raw = upright(raw_ref[...])
    dstep = per_head(dscaled * (xin * xsig), e) - dlog_grad * decay_ref[...]
    graw_ref[...] = flat(dstep * sigmoid(raw))
    waiter(sendbuf.at[pl.ds(0, 63)], disp_ss.at[0], disp_rs.at[0]).wait_send()
    waiter(retbuf.at[pl.ds(0, 63)], ret_ss.at[0], ret_rs.at[0]).wait_send()
    waiter(ybuf.at[pl.ds(0, 2)], a1_s.at[0], a1_r.at[0, 0]).wait_send()
    waiter(ybuf.at[0], a2_s.at[0], a2_r.at[0]).wait_send()
    waiter(rs1_s, r1_s.at[0], r1_r.at[0, 0]).wait_send()
    waiter(rs2_s, r2_s.at[0], r2_r.at[0]).wait_send()
    for d in (0, 1):
        m1(d, 0).wait_send()
        m1(d, 1).wait_send()
        m2(d).wait_send()
        u1(d, 0).wait_send()
        u1(d, 1).wait_send()
        u2(d).wait_send()
    seven(msg_a, sa_s.at[0], sa_r.at[0]).wait_send()
    seven(rec_b, sb_s.at[0], sb_r.at[0]).wait_send()
    seven(msg_c.at[0], sc_s.at[0], sc_r.at[0]).wait_send()
    seven(bmsg_a, sa_s.at[1], sa_r.at[1]).wait_send()
    seven(msg_c.at[1], sc_s.at[1], sc_r.at[1]).wait_send()
    for zz in range(NZ - 1):

        @pl.when(zz < z)
        def _():
            back_send(zz).wait_send()

    for t in range(4):
        n1(t).wait_send()
    for t in range(1, 4):
        n2(t).wait_send()
    seven(turned, t1_s.at[0], t1_r.at[0]).wait_send()
    t2_far(0).wait_send()
    t2_far(1).wait_send()
    six(part, t2_s.at[0], t2_r.at[0]).wait_send()
    six(parts_in, t2_s.at[0], t2_r.at[0]).wait_recv()
    total = part[at_plane(0)].astype(F32)
    for t in (1, -1, 2, -2, 3, -3):
        total += parts_in[at_plane(t)].astype(F32)
    go_ref[...] = total


def fused_call(
    moe_input, cotangent, expert_ids, routing_weights, gate_weight, up_weight, down_weight,
    inner_x, inner_b, inner_c, gate_z, step_raw, decay_rate, skip_weight, norm_gain, w_out,
):
    hbm = pl.BlockSpec(memory_space=pl.ANY)
    dma = pltpu.SemaphoreType.DMA
    V = pltpu.VMEM
    S = pltpu.VMEM
    sems = [dma((16,)), dma((1,)), dma((8,)), dma((1,)), dma((8,))]
    one, each, pairs = dma((1,)), dma((8,)), dma((2, 8))
    sems += [one, pairs, one, each, one, pairs, one, each] + [dma((2, 3))] * 2
    wide = V((128, 1024), F32)
    go, gx, gb, gc, gzz, graw, gwg, uwg, dwg = pl.pallas_call(
        fused_kernel,
        name="fused",
        out_shape=(
            S((32, 1024), F32), S((128, 1024), BF16), S((64, 128), F32), S((64, 128), F32),
            S((128, 1024), BF16), S((16, 128), F32),
            S((NX, 512, 256), BF16), S((NX, 512, 256), BF16), S((256, 2048), BF16),
        ),
        in_specs=[pl.BlockSpec(memory_space=pltpu.HBM)] * 16,
        out_specs=(pl.BlockSpec(memory_space=pltpu.VMEM),) * 9,
        scratch_shapes=[
            V((64, 16, 512), BF16), V((NX, 64, 16, 512), BF16),
            V((NX, 512, 256), BF16), V((NX, 512, 256), BF16), V((256, 2048), BF16),
            V((8, 64, 512), F32), V((2, 8, 64, 512), F32),
            V((2, 8, 32, 512), BF16), V((2, 8, 32, 512), BF16),
            V((2, 8, 64, 512), BF16), V((2, 8, 64, 512), BF16),
            V((64, 16, 512), BF16), V((64, 16, 256), BF16),
            V((64, 16, 256), BF16), V((64, 16, 256), BF16),
            V((NX, 128, 512), BF16),
        ] + sems + [
            V((8, 64, 128), BF16), V((8, 64, 128), BF16), V((64, 128), BF16),
            V((8, 64, 128), BF16), V((64, 128), F32), V((2, 16, 1024), BF16),
            dma((8,)), dma((8,)), dma((2,)), dma((2,)),
            V((2, 128), jnp.int32), V((2, 128), F32), V((128, 512), BF16), V((128, 512), BF16),
            V((128, 1024), BF16), V((64, 128), BF16), V((64, 128), BF16), V((128, 1024), BF16),
            V((16, 128), F32), V((1, 16), F32), V((1, 16), F32), V((1, 1024), F32),
            V((NX, 512, 1024), BF16), wide, wide, wide, wide, V((128, 16), F32),
            V((16, 128), F32), V((128, 128), F32), V((16, 128, 128), F32),
            V((16, 128, 128), BF16), wide, V((64, 1024), BF16), wide,
            V((8, 128, 1024), BF16), wide, V((128, 128), F32), wide, wide, V((128, 128), F32),
            V((8, 80, 128), BF16), V((8, 80, 128), BF16), V((80, 128), BF16),
            V((8, 80, 128), BF16), V((2, 8, 64, 128), BF16), V((2, 8, 64, 128), BF16),
            V((8, 64, 128), F32), V((8, 8, 128), F32),
            V((8, 2, 32, 128), BF16), V((NX, 8, 2, 32, 128), BF16),
            V((8, 32, 1024), BF16), V((8, 32, 1024), BF16),
        ] + [dma((2,))] * 6 + [dma((7,))] * 2 + [dma((1,))] * 4 + [dma((2, 3))] * 2,
        compiler_params=pltpu.CompilerParams(
            collective_id=0, has_side_effects=True, vmem_limit_bytes=62900000
        ),
    )(
        expert_ids.T, routing_weights.T, moe_input, cotangent,
        inner_x, inner_b.T, inner_c.T, gate_z, step_raw.T,
        decay_rate.reshape(1, 16), skip_weight.reshape(1, 16), norm_gain.reshape(1, 1024),
        gate_weight.reshape(NX, 512, 256), up_weight.reshape(NX, 512, 256),
        down_weight.reshape(256, 2048), w_out.reshape(NX, 512, 1024),
    )
    gwg, uwg, dwg, go, gx, gb, gc, gzz, graw = handed_over(
        gwg.reshape(2048, 256), uwg.reshape(2048, 256), dwg, go, gx, gb, gc, gzz, graw
    )
    return gwg[None], uwg[None], dwg[None], go, gx, gb.T, gc.T, gzz, graw.T


def hand_over_kernel(*refs):
    count = (len(refs) - 1) // 2
    srcs, dsts, sem = refs[:count], refs[count : 2 * count], refs[2 * count]
    outs = [pltpu.make_async_copy(srcs[k], dsts[k], sem.at[k]) for k in range(count)]
    for k in range(count):
        outs[k].start()
    for k in range(count):
        outs[k].wait()


def handed_over(*arrays):
    count = len(arrays)
    return pl.pallas_call(
        hand_over_kernel,
        name="handover",
        out_shape=tuple(jax.ShapeDtypeStruct(a.shape, a.dtype) for a in arrays),
        in_specs=[pl.BlockSpec(memory_space=pltpu.VMEM)] * count,
        out_specs=(pl.BlockSpec(memory_space=pl.ANY),) * count,
        scratch_shapes=[pltpu.SemaphoreType.DMA((count,))],
        compiler_params=pltpu.CompilerParams(vmem_limit_bytes=16 * 1024 * 1024),
    )(*arrays)


def solution(mesh):
    finer = Mesh(mesh.devices.reshape(8, 4, 2, mesh.shape["tp"]), ("sp_0", "sp_1", "sp_2", "tp"))
    return jax.shard_map(
        fused_call,
        mesh=finer,
        in_specs=(
            P(SP, "tp"),
            P(SP, "tp"),
            P(SP, None),
            P(SP, None),
            P(SP, None, "tp"),
            P(SP, None, "tp"),
            P(SP, "tp", None),
            P(SP, "tp"),
            P(SP, "tp"),
            P(SP, "tp"),
            P(SP, "tp"),
            P(SP, "tp"),
            P("tp"),
            P("tp"),
            P("tp"),
            P(None, "tp"),
        ),
        out_specs=(
            P(SP, None, "tp"),
            P(SP, None, "tp"),
            P(SP, "tp", None),
            P(SP, "tp"),
            P(SP, "tp"),
            P(SP, "tp"),
            P(SP, "tp"),
            P(SP, "tp"),
            P(SP, "tp"),
        ),
        check_vma=False,
    )
```
